1024 devices in a mesh: dp: 8 (over x), kv: 64 (over z, y), tp: 2 (over core).
Axes of the slice: x: 8, y: 8, z: 8, core: 2. Of those that a mesh axis runs over, the one named last changes fastest.
Arguments:
- tokens: bfloat16 [128, 4096], P('dp', 'kv'), may hold values from -51 to 51
- norm_gain: float32 [4096], P('kv'), may hold values from 0.1 to 1.9
- w_query: bfloat16 [4096, 2048], P('kv', 'tp'), may hold values from -0.09375 to 0.09375
- lambda_head: float32 [16], P('tp'), may hold values from 0.3 to 0.8
- head_gain: float32 [128], replicated, may hold values from 0.1 to 1.9
- w_out: bfloat16 [2048, 4096], P('tp', 'kv'), may hold values from -0.125 to 0.125
- rotated_key_cache: bfloat16 [128, 16384, 128], P('dp', 'kv'), may hold values from -540 to 540, as said below
- value_cache: bfloat16 [128, 16384, 128], P('dp', 'kv'), may hold values from -6 to 6
- lengths: int32 [128], P('dp'), may hold values from 4096 to 16384
Outputs:
- mixed: bfloat16 [128, 4096], P('dp', ('kv', 'tp'))
The draws below stay inside these ranges and needn't reach their ends.
Inputs may be any that keep to these rules, and one draw needn't show every extreme that they name: `rotated_key_cache`: keys have an order-one typical size. The new token is the last filled position, lengths - 1.
All inputs are finite; a program needn't handle non-finite values.
Results may differ from the reference program's by a relative error of at most 0.0112.
Values may be sent and summed in bfloat16 or wider, within the bound.
A program may use at most 32 MiB of HBM per device.

```python
import jax
import jax.numpy as jnp
from jax import lax

D = 4096
HEADS = 16
HEAD_FEATURES = 64
VALUE_DIM = 128
SEQS = 128
CTX = 16384


def draw_tokens(key, part):
    column_scaling = jnp.exp(jnp.log(3.0) * jnp.arange(D, dtype=jnp.float32) / D)
    base = jnp.clip(jax.random.normal(key, (SEQS, D), jnp.float32), -6.0, 6.0)
    values = base * column_scaling[None, :]
    return values.astype(jnp.bfloat16)


def draw_rotated_key_cache(key, part):
    base = jnp.clip(jax.random.normal(key, (SEQS, CTX, 2 * HEAD_FEATURES), jnp.float32), -5.0, 5.0) * 1.8
    return base.astype(jnp.bfloat16)


def set_ends(values, own_key, smallest, largest):
    longest = values.shape.index(max(values.shape))
    spots = []
    for shift in (0, 1):
        where = [jax.random.randint(jax.random.fold_in(own_key, axis), (), 0, length) for axis, length in enumerate(values.shape)]
        where[longest] = (where[longest] + shift) % values.shape[longest]
        spots.append(tuple(where))
    return values.at[spots[0]].set(smallest).at[spots[1]].set(largest)


def block_scale(stream_key, extent, pieces, least, largest):
    level, own = 1.0, jax.random.fold_in(stream_key, 6)
    for dim, blocks in pieces:
        heights = jnp.exp(jax.random.uniform(jax.random.fold_in(own, dim), (blocks,), jnp.float32, least / len(pieces), largest / len(pieces)))
        level = level * jnp.repeat(heights, extent[dim] // blocks).reshape([-1 if axis == dim else 1 for axis in range(len(extent))])
    return level


def noise(key, shape, spread, most, shards=(), kind=jnp.bfloat16):
    values = spread * jax.random.normal(key, shape, jnp.float32)
    if shards:
        values = values * block_scale(key, shape, shards, -0.22, 0.18)
    return jnp.clip(values, -most, most).astype(kind)


def setup_inputs(seed: int = 0) -> dict:
    splits = jax.random.split(jax.random.key(seed), 10)
    return {
        "tokens": draw_tokens(jax.random.fold_in(splits[9], 71), 0),
        "norm_gain": jnp.clip(1.0 + 0.18 * jax.random.normal(splits[1], (D,), jnp.float32), 0.1, 1.9),
        "w_query": noise(splits[2], (D, HEADS * 2 * HEAD_FEATURES), D ** -0.5, 0.09375, ((0, 64), (1, 2))),
        "lambda_head": jnp.clip(0.3 + 0.5 * jax.random.uniform(splits[3], (HEADS,), jnp.float32) ** block_scale(splits[3], (HEADS,), ((0, 2),), -0.2, 0.2), 0.3, 0.8),
        "head_gain": jnp.clip(1.0 + 0.18 * jax.random.normal(splits[4], (VALUE_DIM,), jnp.float32), 0.1, 1.9),
        "w_out": noise(splits[5], (HEADS * VALUE_DIM, D), (HEADS * VALUE_DIM) ** -0.5, 0.125, ((0, 2), (1, 64))),
        "rotated_key_cache": draw_rotated_key_cache(jax.random.fold_in(splits[9], 71), 0),
        "value_cache": noise(splits[7], (SEQS, CTX, VALUE_DIM), 1.0, 6.0, ((0, 8), (1, 64))),
        "lengths": set_ends(jax.random.randint(splits[8], (SEQS,), CTX // 4, CTX + 1), jax.random.fold_in(splits[8], 1), CTX // 4, CTX).astype(jnp.int32),
    }


EPS = 1e-05

def rotate_query(query, position):
    half_dim = query.shape[-1] // 2
    frequency = 1.0 / 10000.0 ** (jnp.arange(half_dim, dtype=jnp.float32) / half_dim)
    angles = position[:, None] * frequency[None, :]
    cosine_table = jnp.concatenate([jnp.cos(angles), jnp.cos(angles)], -1)[:, None, None, :]
    sine_table = jnp.concatenate([jnp.sin(angles), jnp.sin(angles)], -1)[:, None, None, :]
    first_half = query[..., :half_dim]
    second_half = query[..., half_dim:]
    turned = jnp.concatenate([-second_half, first_half], -1)
    return query * cosine_table + turned * sine_table

def finish(numerators, totals, lambdas, head_gain):
    averaged = numerators / totals[..., None]
    head_result = averaged[..., 0, :] - lambdas[..., None] * averaged[..., 1, :]
    factor = lax.rsqrt(lax.optimization_barrier(jnp.mean(head_result * head_result, -1, keepdims=True)) + EPS)
    return (head_result * factor * head_gain).astype(jnp.bfloat16)

def reference(tokens, norm_gain, w_query, lambda_head, head_gain, w_out, rotated_key_cache, value_cache, lengths):
    widened = tokens.astype(jnp.float32)
    squares = lax.optimization_barrier(jnp.sum(widened * widened, -1))
    scale_rows = lax.rsqrt(squares / D + EPS)
    scaled_in = (widened * norm_gain).astype(jnp.bfloat16)
    raw_query = jnp.dot(scaled_in, w_query, preferred_element_type=jnp.float32)
    shaped = (raw_query * scale_rows[:, None]).reshape(SEQS, HEADS, 2, HEAD_FEATURES)
    query = rotate_query(shaped, (lengths - 1).astype(jnp.float32))

    def one_sequence(items):
        query_vector, keys, values, length = items
        keys_sidebyside = keys.astype(jnp.float32).reshape(CTX, 2, HEAD_FEATURES)
        score_rows = jnp.einsum('lxi,wxi->lxw', query_vector, keys_sidebyside, precision=lax.Precision.HIGHEST) * HEAD_FEATURES ** (-0.5)
        valid = jnp.arange(CTX, dtype=jnp.int32) < length
        masked = jnp.where(valid, score_rows, -1e+30)
        maxima = lax.optimization_barrier(jnp.max(masked, -1, keepdims=True))
        weights = jnp.where(valid, jnp.exp(masked - maxima), 0.0)
        totals = lax.optimization_barrier(jnp.sum(weights, -1))
        rounded = lax.optimization_barrier(weights.astype(jnp.bfloat16)).astype(jnp.float32)
        numerators = jnp.einsum('hmp,pv->hmv', rounded, values.astype(jnp.float32))
        return (numerators, totals)
    numerators, totals = lax.map(one_sequence, (query, rotated_key_cache, value_cache, lengths))
    normed = finish(numerators, totals, lambda_head[None, :], head_gain)
    flat = normed.reshape(SEQS, HEADS * VALUE_DIM)
    return jnp.dot(flat, w_out, preferred_element_type=jnp.float32).astype(jnp.bfloat16)
```

```python
import functools

import jax
import jax.numpy as jnp
import numpy as np
from jax import lax
from jax.experimental import pallas as pl
from jax.experimental.pallas import tpu as pltpu
from jax.sharding import PartitionSpec as P

D = 4096
EPS = 1e-05
NEG = -1e30
N = 8
FAR_FIRST = (4, 3, 5, 2, 6, 1, 7)
NEAR_FIRST = (1, 7, 2, 6, 3, 5, 4)
MESH = pl.DeviceIdType.MESH
F32 = jnp.float32
BF16 = jnp.bfloat16


def kernel(
    tok_hbm, gain_hbm, wq_hbm, lam_hbm, hgain_hbm, wo_hbm, k_hbm, v_hbm, len_hbm, freq_hbm,
    out_ref,
    tok, gain, wq, lam, hgain, wo, kc, vc, lens, freq,
    qs, sqs, qr, sqr, zs, zsq, zr, zsqr, gs, gr,
    ns, ss, nr, sr, n2s, s2s, n2r, s2r, fs, fr, full, xs, xr,
    local_sem, send_sem, recv_sem, x_sem,
):
    kv = lax.axis_index("kv")
    tp = lax.axis_index("tp")
    y = lax.rem(kv, N)
    z = lax.div(kv, N)

    def y_id(d):
        return {"kv": z * N + lax.rem(y + d, N)}

    def z_id(d):
        return {"kv": lax.rem(z + d, N) * N + y}

    other = {"tp": 1 - tp}

    barrier = pltpu.get_barrier_semaphore()
    for d in FAR_FIRST:
        pl.semaphore_signal(barrier, inc=1, device_id=y_id(d), device_id_type=MESH)
        pl.semaphore_signal(barrier, inc=1, device_id=z_id(d), device_id_type=MESH)
    pl.semaphore_signal(barrier, inc=1, device_id=other, device_id_type=MESH)

    loads = []
    for i, (src, dst) in enumerate((
        (tok_hbm, tok), (gain_hbm, gain), (wq_hbm, wq), (len_hbm, lens), (freq_hbm, freq),
        (lam_hbm, lam), (hgain_hbm, hgain), (k_hbm, kc), (v_hbm, vc), (wo_hbm, wo),
    )):
        copy = pltpu.make_async_copy(src, dst, local_sem.at[i])
        copy.start()
        loads.append(copy)
    l_tok, l_gain, l_wq, l_len, l_freq, l_lam, l_hgain, l_k, l_v, l_wo = loads

    sends = []

    def send(phase, src, dst, d, ident):
        copy = pltpu.make_async_remote_copy(
            src_ref=src, dst_ref=dst.at[N - d],
            send_sem=send_sem.at[phase, N - d], recv_sem=recv_sem.at[phase, N - d],
            device_id=ident(d), device_id_type=MESH,
        )
        copy.start()
        sends.append(copy)

    def arrived(phase, src, dst, d):
        pltpu.make_async_remote_copy(
            src_ref=src, dst_ref=dst.at[d],
            send_sem=send_sem.at[phase, d], recv_sem=recv_sem.at[phase, d],
            device_id=y_id(0), device_id_type=MESH,
        ).wait_recv()

    l_tok.wait()
    l_gain.wait()
    x = tok[...].astype(F32)
    squares = jnp.broadcast_to(jnp.sum(x * x, -1, keepdims=True), (2 * N, 128))
    for j in range(N):
        sqs[j] = squares[2 * j : 2 * j + 2]
    scaled_in = (x * gain[...]).astype(BF16)
    l_wq.wait()
    partial = jnp.dot(scaled_in, wq[...], preferred_element_type=F32)
    for h in range(8):
        qs[pl.ds(h, 16, stride=8), :] = partial[:, 128 * h : 128 * h + 128]

    def mine(ref, rows):
        return ref[pl.ds(pl.multiple_of(y * rows, rows), rows), :]

    pl.semaphore_wait(barrier, 2 * (N - 1) + 1)
    for d in FAR_FIRST:
        yp = lax.rem(y + d, N)
        send(0, qs.at[pl.ds(pl.multiple_of(yp * 16, 16), 16), :], qr, d, y_id)
        send(1, sqs.at[yp], sqr, d, y_id)

    l_len.wait()
    l_freq.wait()
    lane = lax.broadcasted_iota(jnp.int32, (8, 128), 1)
    tables = []
    for b2 in range(2):
        position = (lens[2 * y + b2] - 1).astype(F32)
        angles = position * jnp.broadcast_to(freq[...], (8, 128))
        tables.append((jnp.cos(angles), jnp.sin(angles)))

    total_q = mine(qs, 16)
    total_sq = sqs[y]
    for d in NEAR_FIRST:
        arrived(0, zs, qr, d)
        total_q = total_q + qr[d]
        arrived(1, zsq, sqr, d)
        total_sq = total_sq + sqr[d]
    zs[...] = total_q
    zsq[...] = total_sq
    for d in FAR_FIRST:
        send(2, zs, zr, d, z_id)
        send(3, zsq, zsqr, d, z_id)
    for d in NEAR_FIRST:
        arrived(2, zs, zr, d)
        total_q = total_q + zr[d]
        arrived(3, zsq, zsqr, d)
        total_sq = total_sq + zsqr[d]
    scale = lax.rsqrt(total_sq / D + EPS)
    own = []
    for b2 in range(2):
        q = total_q[8 * b2 : 8 * b2 + 8] * scale[b2 : b2 + 1]
        turned = jnp.where((lane & 32) == 0, -pltpu.roll(q, 96, 1), pltpu.roll(q, 32, 1))
        cosine, sine = tables[b2]
        q = (q * cosine + turned * sine) * 0.125
        gs[8 * b2 : 8 * b2 + 8, :] = q
        own.append(q)
    for d in FAR_FIRST:
        send(4, gs, gr, d, y_id)

    l_k.wait()
    l_v.wait()
    group = lane // 16
    positions = kv * 256 + lax.broadcasted_iota(jnp.int32, (16, 256), 1)

    def attend(d, queries):
        j = lax.rem(y + d, N)
        stats = jnp.zeros((8, 128), F32)
        for b2 in range(2):
            b = 2 * j + b2
            q = queries[b2]
            rows = jnp.concatenate([jnp.where(lane < 64, q, 0.0), jnp.where(lane < 64, 0.0, q)], 0)
            high = rows.astype(BF16)
            low = (rows - high.astype(F32)).astype(BF16)
            scores = lax.dot_general(
                jnp.concatenate([high, low], 0), kc[b], (((1,), (1,)), ((), ())),
                preferred_element_type=F32,
            )
            scores = scores[:16] + scores[16:]
            valid = positions < lens[b]
            scores = jnp.where(valid, scores, NEG)
            top = jnp.max(scores, -1, keepdims=True)
            weights = jnp.where(valid, jnp.exp(scores - top), 0.0)
            totals = jnp.sum(weights, -1, keepdims=True)
            numer = jnp.dot(weights.astype(BF16), vc[b], preferred_element_type=F32)
            ns[d, 16 * b2 : 16 * b2 + 16, :] = numer.astype(BF16)
            for m in range(2):
                k = 2 * b2 + m
                stats = jnp.where(group == k, top[8 * m : 8 * m + 8], stats)
                stats = jnp.where(group == 4 + k, totals[8 * m : 8 * m + 8], stats)
        ss[d] = stats

    attend(0, own)
    for d in NEAR_FIRST:
        arrived(4, gs, gr, d)
        attend(d, (gr[d, 0:8, :], gr[d, 8:16, :]))
        send(6, ss.at[d], sr, d, y_id)
        send(5, ns.at[d], nr, d, y_id)

    def combined(phase, stats, numer, stat_src, stat_slots, numer_src, numer_slots):
        stat = [stats]
        for d in NEAR_FIRST:
            arrived(phase + 1, stat_src, stat_slots, d)
            stat.append(stat_slots[d])
        top = functools.reduce(jnp.maximum, stat)
        factors = [jnp.exp(s - top) for s in stat]
        total = sum(pltpu.roll(f, 64, 1) * s for f, s in zip(factors, stat))
        sums = [factors[0][:, 16 * k : 16 * k + 1] * numer[8 * k : 8 * k + 8] for k in range(4)]
        for i, d in enumerate(NEAR_FIRST):
            arrived(phase, numer_src, numer_slots, d)
            block = numer_slots[d].astype(F32)
            for k in range(4):
                sums[k] = sums[k] + factors[i + 1][:, 16 * k : 16 * k + 1] * block[8 * k : 8 * k + 8]
        return jnp.where(lane < 64, top, total), sums

    stats, sums = combined(5, ss[0], ns[0].astype(F32), s2s, sr, n2s, nr)
    numer = jnp.concatenate(sums, 0)
    s2s[...] = stats
    n2s[...] = numer.astype(BF16)
    for d in FAR_FIRST:
        send(8, s2s, s2r, d, z_id)
        send(7, n2s, n2r, d, z_id)
    l_lam.wait()
    l_hgain.wait()
    row = lax.broadcasted_iota(jnp.int32, (8, 128), 0)
    lambdas = jnp.zeros((8, 128), F32)
    for h in range(8):
        lambdas = jnp.where(row == h, lam[h], lambdas)
    stats, sums = combined(7, stats, numer, s2s, s2r, n2s, n2r)
    normed = []
    for b2 in range(2):
        first, second = (
            sums[k] / stats[:, 64 + 16 * k : 65 + 16 * k] for k in (2 * b2, 2 * b2 + 1)
        )
        head = first - lambdas * second
        factor = lax.rsqrt(jnp.mean(head * head, -1, keepdims=True) + EPS)
        normed.append(head * factor * hgain[...])
    normed = jnp.concatenate(normed, 0).astype(BF16)
    fs[...] = normed
    for d in FAR_FIRST:
        send(9, fs, fr, d, y_id)
    full[pl.ds(pl.multiple_of(y * 16, 16), 16), :] = normed.astype(F32)
    l_wo.wait()
    for d in NEAR_FIRST:
        arrived(9, fs, fr, d)
        full[pl.ds(pl.multiple_of(lax.rem(y + d, N) * 16, 16), 16), :] = fr[d].astype(F32)
    flat = jnp.concatenate([full[pl.ds(h, 16, stride=8), :] for h in range(8)], 1).astype(BF16)
    mixed = lax.dot_general(flat, wo[...], (((1,), (1,)), ((), ())), preferred_element_type=F32)
    low, high = mixed[:, :32], mixed[:, 32:]
    xs[...] = jnp.where(tp == 0, high, low)
    swap = pltpu.make_async_remote_copy(
        src_ref=xs, dst_ref=xr, send_sem=x_sem.at[0], recv_sem=x_sem.at[1],
        device_id=other, device_id_type=MESH,
    )
    swap.start()
    kept = jnp.where(tp == 0, low, high)
    swap.wait()
    out_ref[...] = (kept + xr[...]).astype(BF16)
    for copy in sends:
        copy.wait_send()


def on_device(tokens, norm_gain, w_query, lambda_head, head_gain, w_out, keys, values, lengths):
    frequency = 1.0 / 10000.0 ** (np.arange(32, dtype=np.float32) / np.float32(32))
    freq = jnp.asarray(np.tile(frequency.astype(np.float32), 4)[None, :])
    operands = (
        tokens, norm_gain[None, :], w_query, lambda_head, head_gain[None, :], w_out.T, keys, values,
        lengths, freq,
    )
    vmem = pltpu.VMEM
    local = [vmem(a.shape, a.dtype) for a in operands]
    local[3] = pltpu.SMEM((8,), F32)
    local[8] = pltpu.SMEM((16,), jnp.int32)
    scratch = local + [
        vmem((128, 128), F32), vmem((N, 2, 128), F32), vmem((N, 16, 128), F32), vmem((N, 2, 128), F32),
        vmem((16, 128), F32), vmem((2, 128), F32), vmem((N, 16, 128), F32), vmem((N, 2, 128), F32),
        vmem((16, 128), F32), vmem((N, 16, 128), F32),
        vmem((N, 32, 128), BF16), vmem((N, 8, 128), F32), vmem((N, 32, 128), BF16), vmem((N, 8, 128), F32),
        vmem((32, 128), BF16), vmem((8, 128), F32), vmem((N, 32, 128), BF16), vmem((N, 8, 128), F32),
        vmem((16, 128), BF16), vmem((N, 16, 128), BF16), vmem((128, 128), F32),
        vmem((16, 32), F32), vmem((16, 32), F32),
        pltpu.SemaphoreType.DMA((10,)), pltpu.SemaphoreType.DMA((10, N)),
        pltpu.SemaphoreType.DMA((10, N)), pltpu.SemaphoreType.DMA((2,)),
    ]
    return pl.pallas_call(
        kernel,
        name="step",
        out_shape=jax.ShapeDtypeStruct((16, 32), BF16),
        in_specs=[pl.BlockSpec(memory_space=pl.ANY)] * len(operands),
        out_specs=pl.BlockSpec(memory_space=pltpu.VMEM),
        scratch_shapes=scratch,
        compiler_params=pltpu.CompilerParams(collective_id=0, has_side_effects=True),
    )(*operands)


def solution(mesh):
    in_specs = (
        P("dp", "kv"),
        P("kv"),
        P("kv", "tp"),
        P("tp"),
        P(),
        P("tp", "kv"),
        P("dp", "kv", None),
        P("dp", "kv", None),
        P("dp"),
    )
    return jax.shard_map(
        on_device, mesh=mesh, in_specs=in_specs, out_specs=P("dp", ("kv", "tp")), check_vma=False
    )
```

```python
import functools

import jax
import jax.numpy as jnp
import numpy as np
from jax import lax
from jax.experimental import pallas as pl
from jax.experimental.pallas import tpu as pltpu
from jax.sharding import PartitionSpec as P

D = 4096
EPS = 1e-05
NEG = -1e30
N = 8
FAR_FIRST = (4, 3, 5, 2, 6, 1, 7)
NEAR_FIRST = (1, 7, 2, 6, 3, 5, 4)
MESH = pl.DeviceIdType.MESH
F32 = jnp.float32
BF16 = jnp.bfloat16


def kernel(
    tok_hbm, gain_hbm, wq_hbm, lam_hbm, hgain_hbm, wo_hbm, k_hbm, v_hbm, len_hbm, freq_hbm,
    out_ref,
    tok, gain, wq, lam, hgain, wo, kc, vc, lens, freq,
    qs, sqs, qr, sqr, zs, zsq, zr, zsqr, gs, gr,
    ns, ss, nr, sr, n2s, s2s, n2r, s2r, fs, fr, full,
    local_sem, send_sem, recv_sem, q_sem, wo_sem,
):
    kv = lax.axis_index("kv")
    tp = lax.axis_index("tp")
    y = lax.rem(kv, N)
    z = lax.div(kv, N)

    def y_id(d):
        return {"kv": z * N + lax.rem(y + d, N), "tp": 1}

    def z_id(d):
        return {"kv": lax.rem(z + d, N) * N + y, "tp": 1}

    def z_id0(d):
        return {"kv": lax.rem(z + d, N) * N + y, "tp": 0}

    barrier = pltpu.get_barrier_semaphore()

    def greet(ident):
        pl.semaphore_signal(barrier, inc=1, device_id=ident, device_id_type=MESH)

    for d in FAR_FIRST:
        greet(z_id(d))

    @pl.when(tp == 1)
    def _():
        for d in FAR_FIRST:
            greet(y_id(d))
        for d in (*FAR_FIRST, 0):
            greet(z_id0(d))

    @pl.when(tp == 0)
    def _():
        greet(z_id(0))

    def load(i, src, dst):
        return pltpu.make_async_copy(src, dst, local_sem.at[i])

    l_tok = load(0, tok_hbm, tok)
    l_gain = load(1, gain_hbm, gain)
    l_wq = load(2, wq_hbm, wq)
    l_wo = load(3, wo_hbm.at[pl.ds(pl.multiple_of(tp * 32, 32), 32), :], wo.at[tp])
    l_len = load(4, len_hbm, lens)
    l_freq = load(5, freq_hbm, freq)
    l_lam = load(6, lam_hbm, lam.at[tp])
    l_hgain = load(7, hgain_hbm, hgain)
    l_k = load(8, k_hbm, kc)
    l_v = load(9, v_hbm, vc)
    for copy in (l_tok, l_gain, l_wq, l_lam):
        copy.start()

    @pl.when(tp == 1)
    def _():
        for copy in (l_len, l_freq, l_hgain, l_k, l_v):
            copy.start()

    l_wo.start()

    def sent(phase, src, dst, d, ident):
        return pltpu.make_async_remote_copy(
            src_ref=src, dst_ref=dst.at[(N - d) % N],
            send_sem=send_sem.at[phase, d], recv_sem=recv_sem.at[phase, (N - d) % N],
            device_id=ident(d), device_id_type=MESH,
        )

    def arrived(phase, src, dst, d):
        pltpu.make_async_remote_copy(
            src_ref=src, dst_ref=dst.at[d],
            send_sem=send_sem.at[phase, d], recv_sem=recv_sem.at[phase, d],
            device_id=z_id0(0), device_id_type=MESH,
        ).wait_recv()

    l_tok.wait()
    l_gain.wait()
    x = tok[...].astype(F32)
    squares = jnp.broadcast_to(jnp.sum(x * x, -1, keepdims=True), (2 * N, 128))
    for j in range(N):
        sqs[j] = squares[2 * j : 2 * j + 2]
    scaled_in = (x * gain[...]).astype(BF16)
    l_wq.wait()
    partial = jnp.dot(scaled_in, wq[...], preferred_element_type=F32)
    for h in range(8):
        qs[pl.ds(h, 16, stride=8), :] = partial[:, 128 * h : 128 * h + 128]

    def query_copy(d):
        zp = lax.rem(z + d, N)
        slot = (N - d) % N
        return pltpu.make_async_remote_copy(
            src_ref=qs.at[pl.ds(pl.multiple_of(zp * 16, 16), 16), :], dst_ref=qr.at[tp, slot],
            send_sem=send_sem.at[0, d], recv_sem=q_sem.at[tp, slot],
            device_id=z_id(d), device_id_type=MESH,
        )

    def square_copy(d):
        return sent(1, sqs.at[lax.rem(z + d, N)], sqr, d, z_id)

    swap_wo = pltpu.make_async_remote_copy(
        src_ref=wo_hbm.at[pl.ds(pl.multiple_of((1 - tp) * 32, 32), 32), :], dst_ref=wo.at[tp],
        send_sem=wo_sem.at[0], recv_sem=wo_sem.at[1],
        device_id={"tp": 1 - tp}, device_id_type=MESH,
    )
    swap_lam = pltpu.make_async_remote_copy(
        src_ref=lam_hbm, dst_ref=lam.at[tp], send_sem=wo_sem.at[2], recv_sem=wo_sem.at[3],
        device_id={"tp": 1 - tp}, device_id_type=MESH,
    )

    @pl.when(tp == 0)
    def _():
        pl.semaphore_wait(barrier, N)

    @pl.when(tp == 1)
    def _():
        pl.semaphore_wait(barrier, 3 * N - 2)

    for d in FAR_FIRST:
        query_copy(d).start()

    @pl.when(tp == 0)
    def _():
        query_copy(0).start()

    @pl.when(tp == 1)
    def _():
        for d in FAR_FIRST:
            square_copy(d).start()

    swap_lam.start()
    swap_wo.start()

    def q_arrived(t, d):
        pltpu.make_async_remote_copy(
            src_ref=gs.at[t], dst_ref=qr.at[t, d],
            send_sem=send_sem.at[0, d], recv_sem=q_sem.at[t, d],
            device_id=z_id0(0), device_id_type=MESH,
        ).wait_recv()

    def exchanges():
        yield [sent(2, zs, zr, d, y_id) for d in FAR_FIRST]
        yield [sent(3, zsq, zsqr, d, y_id) for d in FAR_FIRST]
        yield [sent(4, gs, gr, d, z_id) for d in FAR_FIRST]
        yield [sent(6, ss.at[d], sr, d, z_id) for d in FAR_FIRST]
        yield [sent(5, ns.at[d], nr, d, z_id) for d in FAR_FIRST]
        yield [sent(8, s2s, s2r, d, y_id) for d in FAR_FIRST]
        yield [sent(7, n2s, n2r, d, y_id) for d in FAR_FIRST]

    @pl.when(tp == 1)
    def _():
        l_len.wait()
        l_freq.wait()
        lane = lax.broadcasted_iota(jnp.int32, (8, 128), 1)
        tables = []
        for b2 in range(2):
            position = (lens[2 * z + b2] - 1).astype(F32)
            angles = position * jnp.broadcast_to(freq[...], (8, 128))
            tables.append((jnp.cos(angles), jnp.sin(angles)))

        total_q = [None, qs[pl.ds(pl.multiple_of(z * 16, 16), 16), :]]
        total_sq = sqs[z]
        for d in NEAR_FIRST:
            q_arrived(1, d)
            total_q[1] = total_q[1] + qr[1, d]
            arrived(1, zsq, sqr, d)
            total_sq = total_sq + sqr[d]
        q_arrived(0, 0)
        total_q[0] = qr[0, 0]
        for d in NEAR_FIRST:
            q_arrived(0, d)
            total_q[0] = total_q[0] + qr[0, d]
        for t in range(2):
            zs[t] = total_q[t]
        zsq[...] = total_sq
        for d in FAR_FIRST:
            sent(2, zs, zr, d, y_id).start()
            sent(3, zsq, zsqr, d, y_id).start()
        for d in NEAR_FIRST:
            arrived(2, zs, zr, d)
            for t in range(2):
                total_q[t] = total_q[t] + zr[d, t]
            arrived(3, zsq, zsqr, d)
            total_sq = total_sq + zsqr[d]
        scale = lax.rsqrt(total_sq / D + EPS)
        own = []
        for b2 in range(2):
            cosine, sine = tables[b2]
            for t in range(2):
                q = total_q[t][8 * b2 : 8 * b2 + 8] * scale[b2 : b2 + 1]
                turned = jnp.where((lane & 32) == 0, -pltpu.roll(q, 96, 1), pltpu.roll(q, 32, 1))
                q = (q * cosine + turned * sine) * 0.125
                gs[t, 8 * b2 : 8 * b2 + 8, :] = q
                own.append(q)
        for d in FAR_FIRST:
            sent(4, gs, gr, d, z_id).start()

        l_k.wait()
        l_v.wait()
        group = lane // 8
        positions = kv * 256 + lax.broadcasted_iota(jnp.int32, (32, 256), 1)

        def attend(d, queries):
            j = lax.rem(z + d, N)
            stats = jnp.zeros((8, 128), F32)
            for b2 in range(2):
                b = 2 * j + b2
                q = queries[2 * b2 : 2 * b2 + 2]
                rows = jnp.concatenate(
                    [jnp.where(lane < 64, part, 0.0) for part in q]
                    + [jnp.where(lane < 64, 0.0, part) for part in q], 0
                )
                high = rows.astype(BF16)
                low = (rows - high.astype(F32)).astype(BF16)
                scores = lax.dot_general(
                    jnp.concatenate([high, low], 0), kc[b], (((1,), (1,)), ((), ())),
                    preferred_element_type=F32,
                )
                scores = scores[:32] + scores[32:]
                valid = positions < lens[b]
                scores = jnp.where(valid, scores, NEG)
                top = jnp.max(scores, -1, keepdims=True)
                weights = jnp.where(valid, jnp.exp(scores - top), 0.0)
                totals = jnp.sum(weights, -1, keepdims=True)
                numer = jnp.dot(weights.astype(BF16), vc[b], preferred_element_type=F32)
                ns[d, 32 * b2 : 32 * b2 + 32, :] = numer.astype(BF16)
                for i in range(4):
                    k = 4 * b2 + i
                    stats = jnp.where(group == k, top[8 * i : 8 * i + 8], stats)
                    stats = jnp.where(group == 8 + k, totals[8 * i : 8 * i + 8], stats)
            ss[d] = stats

        attend(0, own)
        for d in NEAR_FIRST:
            arrived(4, gs, gr, d)
            attend(d, [gr[d, t, 8 * b2 : 8 * b2 + 8, :] for b2 in range(2) for t in range(2)])
            sent(6, ss.at[d], sr, d, z_id).start()
            sent(5, ns.at[d], nr, d, z_id).start()

        def combined(phase, stats, numer, stat_src, stat_slots, numer_src, numer_slots):
            stat = [stats]
            for d in NEAR_FIRST:
                arrived(phase + 1, stat_src, stat_slots, d)
                stat.append(stat_slots[d])
            top = functools.reduce(jnp.maximum, stat)
            factors = [jnp.exp(s - top) for s in stat]
            total = sum(pltpu.roll(f, 64, 1) * s for f, s in zip(factors, stat))
            sums = [factors[0][:, 8 * k : 8 * k + 1] * numer[8 * k : 8 * k + 8] for k in range(8)]
            for i, d in enumerate(NEAR_FIRST):
                arrived(phase, numer_src, numer_slots, d)
                block = numer_slots[d].astype(F32)
                for k in range(8):
                    sums[k] = sums[k] + factors[i + 1][:, 8 * k : 8 * k + 1] * block[8 * k : 8 * k + 8]
            return jnp.where(lane < 64, top, total), sums

        stats, sums = combined(5, ss[0], ns[0].astype(F32), s2s, sr, n2s, nr)
        numer = jnp.concatenate(sums, 0)
        s2s[...] = stats
        n2s[...] = numer.astype(BF16)
        for d in FAR_FIRST:
            sent(8, s2s, s2r, d, y_id).start()
            sent(7, n2s, n2r, d, y_id).start()
        l_hgain.wait()
        l_lam.wait()
        swap_lam.wait()
        diagonal = lax.broadcasted_iota(jnp.int32, (8, 8), 0) == lax.broadcasted_iota(jnp.int32, (8, 8), 1)
        lambdas = [
            jnp.sum(jnp.where(diagonal, jnp.broadcast_to(lam[t], (8, 8)), 0.0), -1, keepdims=True)
            for t in range(2)
        ]
        stats, sums = combined(7, stats, numer, s2s, s2r, n2s, n2r)
        normed = []
        for b2 in range(2):
            for t in range(2):
                first, second = (
                    sums[k] / stats[:, 64 + 8 * k : 65 + 8 * k] for k in (4 * b2 + t, 4 * b2 + 2 + t)
                )
                head = first - lambdas[t] * second
                factor = lax.rsqrt(jnp.mean(head * head, -1, keepdims=True) + EPS)
                normed.append(head * factor * hgain[...])
        normed = jnp.concatenate(normed, 0).astype(BF16)
        fs[...] = normed
        sent(10, fs, fr, 0, z_id0).start()
        for d in FAR_FIRST:
            sent(10, fs, fr, d, z_id0).start()
            sent(9, fs, fr, d, z_id).start()
        full[pl.ds(pl.multiple_of(z * 32, 32), 32), :] = normed.astype(F32)

    def gathered(phase, d):
        arrived(phase, fs, fr, d)
        full[pl.ds(pl.multiple_of(lax.rem(z + d, N) * 32, 32), 32), :] = fr[d].astype(F32)

    l_wo.wait()
    swap_wo.wait()

    @pl.when(tp == 1)
    def _():
        for d in NEAR_FIRST:
            gathered(9, d)

    @pl.when(tp == 0)
    def _():
        l_lam.wait()
        swap_lam.wait()
        for d in (0, *NEAR_FIRST):
            gathered(10, d)

    mixed = jnp.zeros((16, 32), F32)
    for t in range(2):
        flat = jnp.concatenate([full[pl.ds(8 * t + h, 16, stride=16), :] for h in range(8)], 1)
        mixed = mixed + lax.dot_general(
            flat.astype(BF16), wo[t], (((1,), (1,)), ((), ())), preferred_element_type=F32
        )
    out_ref[...] = mixed.astype(BF16)

    for d in FAR_FIRST:
        query_copy(d).wait_send()

    @pl.when(tp == 0)
    def _():
        query_copy(0).wait_send()

    @pl.when(tp == 1)
    def _():
        for d in FAR_FIRST:
            square_copy(d).wait_send()
        for copies in exchanges():
            for copy in copies:
                copy.wait_send()
        sent(10, fs, fr, 0, z_id0).wait_send()
        for d in FAR_FIRST:
            sent(10, fs, fr, d, z_id0).wait_send()
            sent(9, fs, fr, d, z_id).wait_send()


def on_device(tokens, norm_gain, w_query, lambda_head, head_gain, w_out, keys, values, lengths):
    frequency = 1.0 / 10000.0 ** (np.arange(32, dtype=np.float32) / np.float32(32))
    freq = jnp.asarray(np.tile(frequency.astype(np.float32), 4)[None, :])
    operands = (
        tokens, norm_gain[None, :], w_query, lambda_head[None, :], head_gain[None, :], w_out.T, keys, values,
        lengths, freq,
    )
    vmem = pltpu.VMEM
    local = [vmem(a.shape, a.dtype) for a in operands]
    local[3] = vmem((2, 1, 8), F32)
    local[5] = vmem((2, 32, 1024), BF16)
    local[8] = pltpu.SMEM((16,), jnp.int32)
    scratch = local + [
        vmem((128, 128), F32), vmem((N, 2, 128), F32), vmem((2, N, 16, 128), F32), vmem((N, 2, 128), F32),
        vmem((2, 16, 128), F32), vmem((2, 128), F32), vmem((N, 2, 16, 128), F32), vmem((N, 2, 128), F32),
        vmem((2, 16, 128), F32), vmem((N, 2, 16, 128), F32),
        vmem((N, 64, 128), BF16), vmem((N, 8, 128), F32), vmem((N, 64, 128), BF16), vmem((N, 8, 128), F32),
        vmem((64, 128), BF16), vmem((8, 128), F32), vmem((N, 64, 128), BF16), vmem((N, 8, 128), F32),
        vmem((32, 128), BF16), vmem((N, 32, 128), BF16), vmem((256, 128), F32),
        pltpu.SemaphoreType.DMA((10,)), pltpu.SemaphoreType.DMA((11, N)),
        pltpu.SemaphoreType.DMA((11, N)), pltpu.SemaphoreType.DMA((2, N)), pltpu.SemaphoreType.DMA((4,)),
    ]
    return pl.pallas_call(
        kernel,
        name="step",
        out_shape=jax.ShapeDtypeStruct((16, 32), BF16),
        in_specs=[pl.BlockSpec(memory_space=pl.ANY)] * len(operands),
        out_specs=pl.BlockSpec(memory_space=pltpu.VMEM),
        scratch_shapes=scratch,
        compiler_params=pltpu.CompilerParams(collective_id=0, has_side_effects=True),
    )(*operands)


def solution(mesh):
    in_specs = (
        P("dp", "kv"),
        P("kv"),
        P("kv", "tp"),
        P("tp"),
        P(),
        P("tp", "kv"),
        P("dp", "kv", None),
        P("dp", "kv", None),
        P("dp"),
    )
    return jax.shard_map(
        on_device, mesh=mesh, in_specs=in_specs, out_specs=P("dp", ("kv", "tp")), check_vma=False
    )
```

```python
import functools

import jax
import jax.numpy as jnp
import numpy as np
from jax import lax
from jax.experimental import pallas as pl
from jax.experimental.pallas import tpu as pltpu
from jax.sharding import PartitionSpec as P

D = 4096
EPS = 1e-05
NEG = -1e30
N = 8
FAR_FIRST = (4, 3, 5, 2, 6, 1, 7)
OWNERS = 7
MESH = pl.DeviceIdType.MESH
F32 = jnp.float32
BF16 = jnp.bfloat16


def kernel(
    tok_hbm, gain_hbm, wq_hbm, lam_hbm, hgain_hbm, wo_hbm, k_hbm, v_hbm, len_hbm, freq_hbm,
    out_ref,
    tok, gain, wq, lam, hgain, wo, kc, vc, lens, freq,
    qs, sqs, qr, sqr, zs, zsq, zr, zsqr, gs, gr,
    ns, ss, nr, sr, n2s, s2s, n2r, s2r, fs, fr, full,
    local_sem, send_sem, recv_sem, piece_sem,
):
    kv = lax.axis_index("kv")
    tp = lax.axis_index("tp")
    y = lax.rem(kv, N)
    z = lax.div(kv, N)
    last = N - 1

    def load(i, src, dst):
        return pltpu.make_async_copy(src, dst, local_sem.at[i])

    l_tok = load(0, tok_hbm, tok)
    l_gain = load(1, gain_hbm, gain)
    l_wq = load(2, wq_hbm, wq)
    l_wo = load(3, wo_hbm.at[pl.ds(pl.multiple_of(tp * 32, 32), 32), :], wo.at[tp])
    l_len = load(4, len_hbm, lens)
    l_freq = load(5, freq_hbm, freq)
    l_lam = load(6, lam_hbm, lam.at[tp])
    l_hgain = load(7, hgain_hbm, hgain)
    l_k = load(8, k_hbm, kc)
    l_v = load(9, v_hbm, vc)
    for copy in (l_tok, l_gain, l_wq):
        copy.start()

    def at(zp, yp, core):
        return {"kv": zp * N + yp, "tp": core}

    def y_id(d):
        return at(z, lax.rem(y + d, N), 1)

    def z_id(d):
        return at(lax.rem(z + d, N), y, 1)

    def z_id0(d):
        return at(lax.rem(z + d, N), y, 0)

    barrier = pltpu.get_barrier_semaphore()

    def greet(ident):
        pl.semaphore_signal(barrier, inc=1, device_id=ident, device_id_type=MESH)

    @pl.when((tp == 1) & (z < last))
    def _():
        for d in FAR_FIRST:
            greet(z_id(d))
            greet(y_id(d))
        for d in range(N):
            greet(z_id0(d))

    @pl.when((tp == 0) | (z == last))
    def _():
        greet({"tp": 1 - tp})

    @pl.when(tp == 1)
    def _():
        for copy in (l_len, l_freq, l_hgain, l_k, l_v):
            copy.start()

    l_lam.start()
    l_wo.start()

    def copy_to(phase, src, dst, ident):
        return pltpu.make_async_remote_copy(
            src_ref=src, dst_ref=dst, send_sem=send_sem.at[phase], recv_sem=recv_sem.at[phase],
            device_id=ident, device_id_type=MESH,
        )

    def arrived(phase, ref):
        copy_to(phase, ref, ref, z_id0(0)).wait_recv()

    def left(phase, ref):
        copy_to(phase, ref, ref, z_id0(0)).wait_send()

    l_tok.wait()
    l_gain.wait()
    x = tok[...].astype(F32)
    scaled_in = (x * gain[...]).astype(BF16)
    l_wq.wait()
    partial = jnp.dot(scaled_in, wq[...], preferred_element_type=F32)
    for h in range(8):
        qs[pl.ds(h, 16, stride=8), :] = partial[:, 128 * h : 128 * h + 128]
    squares = jnp.broadcast_to(jnp.sum(x * x, -1, keepdims=True), (2 * N, 128))
    for j in range(N):
        sqs[j] = squares[2 * j : 2 * j + 2]

    def rows_of(piece):
        if isinstance(piece, int):
            return pl.ds(piece * 16, 16)
        return pl.ds(pl.multiple_of(piece * 16, 16), 16)

    slot = tp * N + z

    def query_copy(d):
        piece = lax.rem(z + d, OWNERS)
        return copy_to(0, qs.at[rows_of(piece), :], qr.at[0, slot], at(piece, y, 1))

    def square_copy(d):
        piece = lax.rem(z + d, OWNERS)
        return copy_to(2, sqs.at[piece], sqr.at[0, z], at(piece, y, 1))

    def last_query_copy():
        return copy_to(1, qs.at[rows_of(last), :], qr.at[1, slot], at(0, y, 1))

    def last_square_copy():
        return copy_to(3, sqs.at[last], sqr.at[1, z], at(0, y, 1))

    other = {"tp": 1 - tp}
    swap_wo = copy_to(
        4, wo_hbm.at[pl.ds(pl.multiple_of((1 - tp) * 32, 32), 32), :], wo.at[tp], other
    )
    swap_lam = copy_to(5, lam_hbm, lam.at[tp], other)

    @pl.when(tp == 0)
    def _():
        pl.semaphore_wait(barrier, jnp.where(z == last, N, N - 1))

    @pl.when(tp == 1)
    def _():
        pl.semaphore_wait(barrier, jnp.where(z == last, N, 2 * N - 2))

    ORDER = (4, 3, 5, 2, 6, 1)
    for d in ORDER:
        query_copy(d).start()

    @pl.when((tp == 0) | (z == last))
    def _():
        query_copy(0).start()

    @pl.when((tp == 0) | (z > 0))
    def _():
        last_query_copy().start()

    @pl.when(tp == 1)
    def _():
        for d in ORDER:
            square_copy(d).start()

        @pl.when(z == last)
        def _():
            square_copy(0).start()

        @pl.when(z > 0)
        def _():
            last_square_copy().start()

    swap_lam.start()
    swap_wo.start()

    @pl.when(tp == 1)
    def _():
        lane = lax.broadcasted_iota(jnp.int32, (8, 128), 1)
        l_len.wait()
        l_freq.wait()

        def tables_of(piece):
            tables = []
            for b2 in range(2):
                position = (lens[2 * piece + b2] - 1).astype(F32)
                angles = position * jnp.broadcast_to(freq[...], (8, 128))
                tables.append((jnp.cos(angles), jnp.sin(angles)))
            return tables

        def plane_sum(i, piece):
            qr[i, N + z] = qs[rows_of(piece), :]
            sqr[i, z] = sqs[piece]
            arrived(i, qr.at[i, pl.ds(0, 2 * N - 1)])
            arrived(2 + i, sqr.at[i, pl.ds(0, N - 1)])
            for t in range(2):
                zs[i, t] = functools.reduce(lambda a, b: a + b, [qr[i, N * t + k] for k in range(N)])
            zsq[i] = functools.reduce(lambda a, b: a + b, [sqr[i, k] for k in range(N)])
            for d in FAR_FIRST:
                copy_to(6 + i, zs.at[i], zr.at[i, N - d], y_id(d)).start()
                copy_to(8 + i, zsq.at[i], zsqr.at[i, N - d], y_id(d)).start()

        def finished(i, piece, tables):
            arrived(6 + i, zr.at[i, pl.ds(1, N - 1)])
            arrived(8 + i, zsqr.at[i, pl.ds(1, N - 1)])
            total_sq = functools.reduce(lambda a, b: a + b, [zsqr[i, k] for k in range(1, N)], zsq[i])
            scale = lax.rsqrt(total_sq / D + EPS)
            for t in range(2):
                total = functools.reduce(lambda a, b: a + b, [zr[i, k, t] for k in range(1, N)], zs[i, t])
                for b2 in range(2):
                    cosine, sine = tables[b2]
                    q = total[8 * b2 : 8 * b2 + 8] * scale[b2 : b2 + 1]
                    turned = jnp.where((lane & 32) == 0, -pltpu.roll(q, 96, 1), pltpu.roll(q, 32, 1))
                    q = (q * cosine + turned * sine) * 0.125
                    gs[i, t, 8 * b2 : 8 * b2 + 8, :] = q
                    gr[piece, t, 8 * b2 : 8 * b2 + 8, :] = q
            for d in FAR_FIRST:
                pltpu.make_async_remote_copy(
                    src_ref=gs.at[i], dst_ref=gr.at[piece], send_sem=send_sem.at[10 + i],
                    recv_sem=piece_sem.at[piece], device_id=z_id(d), device_id_type=MESH,
                ).start()

        @pl.when((z > 0) & (z < last))
        def _():
            tables = tables_of(z)
            plane_sum(0, z)
            finished(0, z, tables)

        @pl.when(z == 0)
        def _():
            tables = tables_of(0)
            last_tables = tables_of(last)
            plane_sum(0, 0)
            plane_sum(1, last)
            finished(0, 0, tables)
            finished(1, last, last_tables)

        l_k.wait()
        l_v.wait()
        group = lane // 8
        positions = kv * 256 + lax.broadcasted_iota(jnp.int32, (32, 256), 1)

        def attend(d):
            piece = lax.rem(z + d, N)

            @pl.when(((piece != z) | (z == last)) & ((piece != last) | (z != 0)))
            def _():
                pltpu.make_async_remote_copy(
                    src_ref=gs.at[0], dst_ref=gr.at[piece], send_sem=send_sem.at[10],
                    recv_sem=piece_sem.at[piece], device_id=z_id0(0), device_id_type=MESH,
                ).wait_recv()

            stats = jnp.zeros((8, 128), F32)
            for b2 in range(2):
                b = 2 * piece + b2
                q = [gr[piece, t, 8 * b2 : 8 * b2 + 8, :] for t in range(2)]
                rows = jnp.concatenate(
                    [jnp.where(lane < 64, part, 0.0) for part in q]
                    + [jnp.where(lane < 64, 0.0, part) for part in q], 0
                )
                high = rows.astype(BF16)
                low = (rows - high.astype(F32)).astype(BF16)
                scores = lax.dot_general(
                    jnp.concatenate([high, low], 0), kc[b], (((1,), (1,)), ((), ())),
                    preferred_element_type=F32,
                )
                scores = scores[:32] + scores[32:]
                valid = positions < lens[b]
                scores = jnp.where(valid, scores, NEG)
                top = jnp.max(scores, -1, keepdims=True)
                weights = jnp.where(valid, jnp.exp(scores - top), 0.0)
                totals = jnp.sum(weights, -1, keepdims=True)
                numer = jnp.dot(weights.astype(BF16), vc[b], preferred_element_type=F32)
                ns[d, 32 * b2 : 32 * b2 + 32, :] = numer.astype(BF16)
                for i in range(4):
                    k = 4 * b2 + i
                    stats = jnp.where(group == k, top[8 * i : 8 * i + 8], stats)
                    stats = jnp.where(group == 8 + k, totals[8 * i : 8 * i + 8], stats)
            ss[d] = stats
            if d:
                copy_to(12, ss.at[d], sr.at[N - d], z_id(d)).start()
                copy_to(13, ns.at[d], nr.at[N - d], z_id(d)).start()

        for d in (0, 7, 1, 6, 2, 5, 3, 4):
            attend(d)

        def combined(phase, stats, numer, stat_slots, numer_slots):
            arrived(phase, stat_slots.at[pl.ds(1, N - 1)])
            stat = [stats] + [stat_slots[k] for k in range(1, N)]
            top = functools.reduce(jnp.maximum, stat)
            factors = [jnp.exp(s - top) for s in stat]
            total = sum(pltpu.roll(f, 64, 1) * s for f, s in zip(factors, stat))
            arrived(phase + 1, numer_slots.at[pl.ds(1, N - 1)])
            sums = [factors[0][:, 8 * k : 8 * k + 1] * numer[8 * k : 8 * k + 8] for k in range(8)]
            for i in range(1, N):
                block = numer_slots[i].astype(F32)
                for k in range(8):
                    sums[k] = sums[k] + factors[i][:, 8 * k : 8 * k + 1] * block[8 * k : 8 * k + 8]
            return jnp.where(lane < 64, top, total), sums

        stats, sums = combined(12, ss[0], ns[0].astype(F32), sr, nr)
        numer = jnp.concatenate(sums, 0)
        s2s[...] = stats
        n2s[...] = numer.astype(BF16)
        for d in FAR_FIRST:
            copy_to(14, s2s, s2r.at[N - d], y_id(d)).start()
            copy_to(15, n2s, n2r.at[N - d], y_id(d)).start()
        l_hgain.wait()
        l_lam.wait()
        arrived(5, lam.at[0])
        diagonal = lax.broadcasted_iota(jnp.int32, (8, 8), 0) == lax.broadcasted_iota(jnp.int32, (8, 8), 1)
        lambdas = [
            jnp.sum(jnp.where(diagonal, jnp.broadcast_to(lam[t], (8, 8)), 0.0), -1, keepdims=True)
            for t in range(2)
        ]
        stats, sums = combined(14, stats, numer, s2r, n2r)
        normed = []
        for b2 in range(2):
            for t in range(2):
                first, second = (
                    sums[k] / stats[:, 64 + 8 * k : 65 + 8 * k] for k in (4 * b2 + t, 4 * b2 + 2 + t)
                )
                head = first - lambdas[t] * second
                factor = lax.rsqrt(jnp.mean(head * head, -1, keepdims=True) + EPS)
                normed.append(head * factor * hgain[...])
        normed = jnp.concatenate(normed, 0).astype(BF16)
        fs[...] = normed
        for d in FAR_FIRST:
            copy_to(16, fs, fr.at[N - d], z_id0(d)).start()
            copy_to(16, fs, fr.at[N - d], z_id(d)).start()
        copy_to(16, fs, fr.at[0], z_id0(0)).start()
        fr[0] = normed

    @pl.when(tp == 1)
    def _():
        arrived(16, fr.at[pl.ds(1, N - 1)])

    @pl.when(tp == 0)
    def _():
        l_lam.wait()
        arrived(5, lam.at[0])
        arrived(16, fr)

    l_wo.wait()
    arrived(4, wo.at[0])
    for d in range(N):
        full[pl.ds(pl.multiple_of(lax.rem(z + d, N) * 32, 32), 32), :] = fr[d].astype(F32)
    mixed = jnp.zeros((16, 32), F32)
    for t in range(2):
        flat = jnp.concatenate([full[pl.ds(8 * t + h, 16, stride=16), :] for h in range(8)], 1)
        mixed = mixed + lax.dot_general(
            flat.astype(BF16), wo[t], (((1,), (1,)), ((), ())), preferred_element_type=F32
        )
    out_ref[...] = mixed.astype(BF16)

    left(4, wo.at[0])
    left(5, lam.at[0])
    @pl.when((tp == 0) | (z == last))
    def _():
        left(0, qr.at[0, pl.ds(0, OWNERS)])

    @pl.when((tp == 1) & (z < last))
    def _():
        left(0, qr.at[0, pl.ds(0, OWNERS - 1)])

    @pl.when((tp == 0) | (z > 0))
    def _():
        left(1, qr.at[1, 0])

    @pl.when(tp == 1)
    def _():
        @pl.when(z == last)
        def _():
            left(2, sqr.at[0, pl.ds(0, OWNERS)])

        @pl.when(z < last)
        def _():
            left(2, sqr.at[0, pl.ds(0, OWNERS - 1)])
            left(6, zr.at[0, pl.ds(1, N - 1)])
            left(8, zsqr.at[0, pl.ds(1, N - 1)])
            left(10, gr.at[pl.ds(1, N - 1)])

        @pl.when(z > 0)
        def _():
            left(3, sqr.at[1, 0])

        @pl.when(z == 0)
        def _():
            left(7, zr.at[1, pl.ds(1, N - 1)])
            left(9, zsqr.at[1, pl.ds(1, N - 1)])
            left(11, gr.at[pl.ds(1, N - 1)])

        left(12, sr.at[pl.ds(1, N - 1)])
        left(13, nr.at[pl.ds(1, N - 1)])
        left(14, s2r.at[pl.ds(1, N - 1)])
        left(15, n2r.at[pl.ds(1, N - 1)])
        left(16, fr.at[pl.ds(1, N - 1)])
        left(16, fr)


def on_device(tokens, norm_gain, w_query, lambda_head, head_gain, w_out, keys, values, lengths):
    frequency = 1.0 / 10000.0 ** (np.arange(32, dtype=np.float32) / np.float32(32))
    freq = jnp.asarray(np.tile(frequency.astype(np.float32), 4)[None, :])
    operands = (
        tokens, norm_gain[None, :], w_query, lambda_head[None, :], head_gain[None, :], w_out.T, keys, values,
        lengths, freq,
    )
    vmem = pltpu.VMEM
    local = [vmem(a.shape, a.dtype) for a in operands]
    local[3] = vmem((2, 1, 8), F32)
    local[5] = vmem((2, 32, 1024), BF16)
    local[8] = pltpu.SMEM((16,), jnp.int32)
    scratch = local + [
        vmem((128, 128), F32), vmem((N, 2, 128), F32),
        vmem((2, 2 * N, 16, 128), F32), vmem((2, N, 2, 128), F32),
        vmem((2, 2, 16, 128), F32), vmem((2, 2, 128), F32),
        vmem((2, N, 2, 16, 128), F32), vmem((2, N, 2, 128), F32),
        vmem((2, 2, 16, 128), F32), vmem((N, 2, 16, 128), F32),
        vmem((N, 64, 128), BF16), vmem((N, 8, 128), F32), vmem((N, 64, 128), BF16), vmem((N, 8, 128), F32),
        vmem((64, 128), BF16), vmem((8, 128), F32), vmem((N, 64, 128), BF16), vmem((N, 8, 128), F32),
        vmem((32, 128), BF16), vmem((N, 32, 128), BF16), vmem((256, 128), F32),
        pltpu.SemaphoreType.DMA((10,)), pltpu.SemaphoreType.DMA((17,)), pltpu.SemaphoreType.DMA((17,)),
        pltpu.SemaphoreType.DMA((N,)),
    ]
    return pl.pallas_call(
        kernel,
        name="step",
        out_shape=jax.ShapeDtypeStruct((16, 32), BF16),
        in_specs=[pl.BlockSpec(memory_space=pl.ANY)] * len(operands),
        out_specs=pl.BlockSpec(memory_space=pltpu.VMEM),
        scratch_shapes=scratch,
        compiler_params=pltpu.CompilerParams(collective_id=0, has_side_effects=True),
    )(*operands)


def solution(mesh):
    in_specs = (
        P("dp", "kv"),
        P("kv"),
        P("kv", "tp"),
        P("tp"),
        P(),
        P("tp", "kv"),
        P("dp", "kv", None),
        P("dp", "kv", None),
        P("dp"),
    )
    return jax.shard_map(
        on_device, mesh=mesh, in_specs=in_specs, out_specs=P("dp", ("kv", "tp")), check_vma=False
    )
```

```python
import functools

import jax
import jax.numpy as jnp
import numpy as np
from jax import lax
from jax.experimental import pallas as pl
from jax.experimental.pallas import tpu as pltpu
from jax.sharding import PartitionSpec as P

D = 4096
EPS = 1e-05
NEG = -1e30
N = 8
FAR_FIRST = (4, 3, 5, 2, 6, 1, 7)
OWNERS = 7
MESH = pl.DeviceIdType.MESH
F32 = jnp.float32
BF16 = jnp.bfloat16


def kernel(
    tok_hbm, gain_hbm, wq_hbm, lam_hbm, hgain_hbm, wo_hbm, k_hbm, v_hbm, len_hbm, freq_hbm,
    out_ref,
    tok, gain, wq, lam, hgain, wo, kc, vc, lens, freq,
    qs, sqs, qr, sqr, zs, zsq, zr, zsqr, gs, gr,
    ns, ss, nr, sr, n2s, s2s, n2r, s2r, fs, fr, full,
    local_sem, send_sem, recv_sem, piece_sem,
):
    kv = lax.axis_index("kv")
    tp = lax.axis_index("tp")
    y = lax.rem(kv, N)
    z = lax.div(kv, N)
    last = N - 1

    def load(i, src, dst):
        return pltpu.make_async_copy(src, dst, local_sem.at[i])

    l_tok = load(0, tok_hbm, tok)
    l_gain = load(1, gain_hbm, gain)
    l_wq = load(2, wq_hbm, wq)
    l_wo = load(3, wo_hbm.at[pl.ds(pl.multiple_of(tp * 32, 32), 32), :], wo.at[tp])
    l_len = load(4, len_hbm, lens)
    l_freq = load(5, freq_hbm, freq)
    l_lam = load(6, lam_hbm, lam.at[tp])
    l_hgain = load(7, hgain_hbm, hgain)
    l_k = load(8, k_hbm, kc)
    l_v = load(9, v_hbm, vc)
    for copy in (l_tok, l_gain, l_wq):
        copy.start()

    def at(zp, yp, core):
        return {"kv": zp * N + yp, "tp": core}

    def y_id(d):
        return at(z, lax.rem(y + d, N), 1)

    def z_id(d):
        return at(lax.rem(z + d, N), y, 1)

    def z_id0(d):
        return at(lax.rem(z + d, N), y, 0)

    barrier = pltpu.get_barrier_semaphore()

    def greet(ident):
        pl.semaphore_signal(barrier, inc=1, device_id=ident, device_id_type=MESH)

    @pl.when((tp == 1) & (z < last))
    def _():
        for d in FAR_FIRST:
            greet(z_id(d))
            greet(y_id(d))
        for d in range(N):
            greet(z_id0(d))

    @pl.when((tp == 0) | (z == last))
    def _():
        greet({"tp": 1 - tp})

    @pl.when(tp == 1)
    def _():
        for copy in (l_len, l_freq, l_hgain, l_k, l_v):
            copy.start()

    l_lam.start()
    l_wo.start()

    def copy_to(phase, src, dst, ident):
        return pltpu.make_async_remote_copy(
            src_ref=src, dst_ref=dst, send_sem=send_sem.at[phase], recv_sem=recv_sem.at[phase],
            device_id=ident, device_id_type=MESH,
        )

    def arrived(phase, ref):
        copy_to(phase, ref, ref, z_id0(0)).wait_recv()

    def left(phase, ref):
        copy_to(phase, ref, ref, z_id0(0)).wait_send()

    l_tok.wait()
    l_gain.wait()
    x = tok[...].astype(F32)
    scaled_in = (x * gain[...]).astype(BF16)
    l_wq.wait()
    partial = jnp.dot(scaled_in, wq[...], preferred_element_type=F32)
    for h in range(8):
        qs[pl.ds(h, 16, stride=8), :] = partial[:, 128 * h : 128 * h + 128]
    squares = jnp.broadcast_to(jnp.sum(x * x, -1, keepdims=True), (2 * N, 128))
    for j in range(N):
        sqs[j] = squares[2 * j : 2 * j + 2]

    def rows_of(piece):
        if isinstance(piece, int):
            return pl.ds(piece * 16, 16)
        return pl.ds(pl.multiple_of(piece * 16, 16), 16)

    slot = tp * N + z

    def query_copy(d):
        piece = lax.rem(z + d, OWNERS)
        return copy_to(0, qs.at[rows_of(piece), :], qr.at[0, slot], at(piece, y, 1))

    def square_copy(d):
        piece = lax.rem(z + d, OWNERS)
        return copy_to(2, sqs.at[piece], sqr.at[0, z], at(piece, y, 1))

    def last_query_copy():
        return copy_to(1, qs.at[rows_of(last), :], qr.at[1, slot], at(0, y, 1))

    def last_square_copy():
        return copy_to(3, sqs.at[last], sqr.at[1, z], at(0, y, 1))

    other = {"tp": 1 - tp}
    swap_wo = copy_to(
        4, wo_hbm.at[pl.ds(pl.multiple_of((1 - tp) * 32, 32), 32), :], wo.at[tp], other
    )
    swap_lam = copy_to(5, lam_hbm, lam.at[tp], other)

    @pl.when(tp == 0)
    def _():
        pl.semaphore_wait(barrier, jnp.where(z == last, N, N - 1))

    @pl.when(tp == 1)
    def _():
        pl.semaphore_wait(barrier, jnp.where(z == last, N, 2 * N - 2))

    ORDER = (4, 3, 5, 2, 6, 1)
    for d in ORDER:
        query_copy(d).start()

    @pl.when((tp == 0) | (z == last))
    def _():
        query_copy(0).start()

    @pl.when((tp == 0) | (z > 0))
    def _():
        last_query_copy().start()

    @pl.when(tp == 1)
    def _():
        for d in ORDER:
            square_copy(d).start()

        @pl.when(z == last)
        def _():
            square_copy(0).start()

        @pl.when(z > 0)
        def _():
            last_square_copy().start()

    swap_lam.start()
    swap_wo.start()

    @pl.when(tp == 1)
    def _():
        lane = lax.broadcasted_iota(jnp.int32, (8, 128), 1)
        l_len.wait()
        l_freq.wait()

        def tables_of(piece):
            tables = []
            for b2 in range(2):
                position = (lens[2 * piece + b2] - 1).astype(F32)
                angles = position * jnp.broadcast_to(freq[...], (8, 128))
                tables.append((jnp.cos(angles), jnp.sin(angles)))
            return tables

        def plane_sum(i, piece):
            qr[i, N + z] = qs[rows_of(piece), :]
            sqr[i, z] = sqs[piece]
            arrived(i, qr.at[i, pl.ds(0, 2 * N - 1)])
            arrived(2 + i, sqr.at[i, pl.ds(0, N - 1)])
            for t in range(2):
                zs[i, t] = functools.reduce(lambda a, b: a + b, [qr[i, N * t + k] for k in range(N)])
            zsq[i] = functools.reduce(lambda a, b: a + b, [sqr[i, k] for k in range(N)])
            for d in FAR_FIRST:
                copy_to(6 + i, zs.at[i], zr.at[i, N - d], y_id(d)).start()
                copy_to(8 + i, zsq.at[i], zsqr.at[i, N - d], y_id(d)).start()

        def finished(i, piece, tables):
            arrived(6 + i, zr.at[i, pl.ds(1, N - 1)])
            arrived(8 + i, zsqr.at[i, pl.ds(1, N - 1)])
            total_sq = functools.reduce(lambda a, b: a + b, [zsqr[i, k] for k in range(1, N)], zsq[i])
            scale = lax.rsqrt(total_sq / D + EPS)
            for t in range(2):
                total = functools.reduce(lambda a, b: a + b, [zr[i, k, t] for k in range(1, N)], zs[i, t])
                for b2 in range(2):
                    cosine, sine = tables[b2]
                    q = total[8 * b2 : 8 * b2 + 8] * scale[b2 : b2 + 1]
                    turned = jnp.where((lane & 32) == 0, -pltpu.roll(q, 96, 1), pltpu.roll(q, 32, 1))
                    q = (q * cosine + turned * sine) * 0.125
                    gs[i, t, 8 * b2 : 8 * b2 + 8, :] = q
                    gr[piece, t, 8 * b2 : 8 * b2 + 8, :] = q
            for d in FAR_FIRST:
                pltpu.make_async_remote_copy(
                    src_ref=gs.at[i], dst_ref=gr.at[piece], send_sem=send_sem.at[10 + i],
                    recv_sem=piece_sem.at[piece], device_id=z_id(d), device_id_type=MESH,
                ).start()

        @pl.when((z > 0) & (z < last))
        def _():
            tables = tables_of(z)
            plane_sum(0, z)
            finished(0, z, tables)

        @pl.when(z == 0)
        def _():
            tables = tables_of(0)
            last_tables = tables_of(last)
            plane_sum(0, 0)
            plane_sum(1, last)
            finished(0, 0, tables)
            finished(1, last, last_tables)

        l_k.wait()
        l_v.wait()
        group = lane // 8
        positions = kv * 256 + lax.broadcasted_iota(jnp.int32, (32, 256), 1)

        def attend(d):
            piece = lax.rem(z + d, N)

            @pl.when(((piece != z) | (z == last)) & ((piece != last) | (z != 0)))
            def _():
                pltpu.make_async_remote_copy(
                    src_ref=gs.at[0], dst_ref=gr.at[piece], send_sem=send_sem.at[10],
                    recv_sem=piece_sem.at[piece], device_id=z_id0(0), device_id_type=MESH,
                ).wait_recv()

            stats = jnp.zeros((8, 128), F32)
            for b2 in range(2):
                b = 2 * piece + b2
                q = [gr[piece, t, 8 * b2 : 8 * b2 + 8, :] for t in range(2)]
                rows = jnp.concatenate(
                    [jnp.where(lane < 64, part, 0.0) for part in q]
                    + [jnp.where(lane < 64, 0.0, part) for part in q], 0
                )
                high = rows.astype(BF16)
                low = (rows - high.astype(F32)).astype(BF16)
                scores = lax.dot_general(
                    jnp.concatenate([high, low], 0), kc[b], (((1,), (1,)), ((), ())),
                    preferred_element_type=F32,
                )
                scores = scores[:32] + scores[32:]
                valid = positions < lens[b]
                scores = jnp.where(valid, scores, NEG)
                top = jnp.max(scores, -1, keepdims=True)
                weights = jnp.where(valid, jnp.exp(scores - top), 0.0)
                totals = jnp.sum(weights, -1, keepdims=True)
                numer = jnp.dot(weights.astype(BF16), vc[b], preferred_element_type=F32)
                ns[d, 32 * b2 : 32 * b2 + 32, :] = numer.astype(BF16)
                for i in range(4):
                    k = 4 * b2 + i
                    stats = jnp.where(group == k, top[8 * i : 8 * i + 8], stats)
                    stats = jnp.where(group == 8 + k, totals[8 * i : 8 * i + 8], stats)
            ss[d] = stats
            if d:
                copy_to(12, ss.at[d], sr.at[N - d], z_id(d)).start()
                copy_to(13, ns.at[d], nr.at[N - d], z_id(d)).start()

        for d in (0, 7, 1, 6, 2, 5, 3, 4):
            attend(d)

        def combined(phase, stats, numer, stat_slots, numer_slots):
            arrived(phase, stat_slots.at[pl.ds(1, N - 1)])
            stat = [stats] + [stat_slots[k] for k in range(1, N)]
            top = functools.reduce(jnp.maximum, stat)
            factors = [jnp.exp(s - top) for s in stat]
            total = sum(pltpu.roll(f, 64, 1) * s for f, s in zip(factors, stat))
            arrived(phase + 1, numer_slots.at[pl.ds(1, N - 1)])
            sums = [factors[0][:, 8 * k : 8 * k + 1] * numer[8 * k : 8 * k + 8] for k in range(8)]
            for i in range(1, N):
                block = numer_slots[i].astype(F32)
                for k in range(8):
                    sums[k] = sums[k] + factors[i][:, 8 * k : 8 * k + 1] * block[8 * k : 8 * k + 8]
            return jnp.where(lane < 64, top, total), sums

        stats, sums = combined(12, ss[0], ns[0].astype(F32), sr, nr)
        numer = jnp.concatenate(sums, 0)
        s2s[...] = stats
        n2s[...] = numer.astype(BF16)
        for d in FAR_FIRST:
            copy_to(14, s2s, s2r.at[N - d], y_id(d)).start()
            copy_to(15, n2s, n2r.at[N - d], y_id(d)).start()
        l_hgain.wait()
        l_lam.wait()
        arrived(5, lam.at[0])
        diagonal = lax.broadcasted_iota(jnp.int32, (8, 8), 0) == lax.broadcasted_iota(jnp.int32, (8, 8), 1)
        lambdas = [
            jnp.sum(jnp.where(diagonal, jnp.broadcast_to(lam[t], (8, 8)), 0.0), -1, keepdims=True)
            for t in range(2)
        ]
        stats, sums = combined(14, stats, numer, s2r, n2r)
        normed = []
        for b2 in range(2):
            for t in range(2):
                first, second = (
                    sums[k] / stats[:, 64 + 8 * k : 65 + 8 * k] for k in (4 * b2 + t, 4 * b2 + 2 + t)
                )
                head = first - lambdas[t] * second
                factor = lax.rsqrt(jnp.mean(head * head, -1, keepdims=True) + EPS)
                normed.append(head * factor * hgain[...])
        normed = jnp.concatenate(normed, 0).astype(BF16)
        fs[...] = normed
        for d in FAR_FIRST:
            copy_to(16, fs, fr.at[N - d], z_id0(d)).start()
            copy_to(16, fs, fr.at[N - d], z_id(d)).start()
        copy_to(16, fs, fr.at[0], z_id0(0)).start()
        fr[0] = normed

    @pl.when(tp == 1)
    def _():
        arrived(16, fr.at[pl.ds(1, N - 1)])

    @pl.when(tp == 0)
    def _():
        l_lam.wait()
        arrived(5, lam.at[0])
        arrived(16, fr)

    l_wo.wait()
    arrived(4, wo.at[0])
    for d in range(N):
        full[pl.ds(pl.multiple_of(lax.rem(z + d, N) * 32, 32), 32), :] = fr[d].astype(F32)
    mixed = jnp.zeros((16, 32), F32)
    for t in range(2):
        flat = jnp.concatenate([full[pl.ds(8 * t + h, 16, stride=16), :] for h in range(8)], 1)
        mixed = mixed + lax.dot_general(
            flat.astype(BF16), wo[t], (((1,), (1,)), ((), ())), preferred_element_type=F32
        )
    out_ref[...] = mixed.astype(BF16)

    left(4, wo.at[0])
    left(5, lam.at[0])
    @pl.when((tp == 0) | (z == last))
    def _():
        left(0, qr.at[0, pl.ds(0, OWNERS)])

    @pl.when((tp == 1) & (z < last))
    def _():
        left(0, qr.at[0, pl.ds(0, OWNERS - 1)])

    @pl.when((tp == 0) | (z > 0))
    def _():
        left(1, qr.at[1, 0])

    @pl.when(tp == 1)
    def _():
        @pl.when(z == last)
        def _():
            left(2, sqr.at[0, pl.ds(0, OWNERS)])

        @pl.when(z < last)
        def _():
            left(2, sqr.at[0, pl.ds(0, OWNERS - 1)])
            left(6, zr.at[0, pl.ds(1, N - 1)])
            left(8, zsqr.at[0, pl.ds(1, N - 1)])
            left(10, gr.at[pl.ds(1, N - 1)])

        @pl.when(z > 0)
        def _():
            left(3, sqr.at[1, 0])

        @pl.when(z == 0)
        def _():
            left(7, zr.at[1, pl.ds(1, N - 1)])
            left(9, zsqr.at[1, pl.ds(1, N - 1)])
            left(11, gr.at[pl.ds(1, N - 1)])

        left(12, sr.at[pl.ds(1, N - 1)])
        left(13, nr.at[pl.ds(1, N - 1)])
        left(14, s2r.at[pl.ds(1, N - 1)])
        left(15, n2r.at[pl.ds(1, N - 1)])
        left(16, fr.at[pl.ds(1, N - 1)])
        left(16, fr)


def on_device(tokens, norm_gain, w_query, lambda_head, head_gain, w_out, keys, values, lengths):
    frequency = 1.0 / 10000.0 ** (np.arange(32, dtype=np.float32) / np.float32(32))
    freq = jnp.asarray(np.tile(frequency.astype(np.float32), 4)[None, :])
    operands = (
        tokens, norm_gain[None, :], w_query, lambda_head[None, :], head_gain[None, :], w_out.T, keys, values,
        lengths, freq,
    )
    vmem = pltpu.VMEM
    local = [vmem(a.shape, a.dtype) for a in operands]
    local[3] = vmem((2, 1, 8), F32)
    local[5] = vmem((2, 32, 1024), BF16)
    local[8] = pltpu.SMEM((16,), jnp.int32)
    scratch = local + [
        vmem((128, 128), F32), vmem((N, 2, 128), F32),
        vmem((2, 2 * N, 16, 128), F32), vmem((2, N, 2, 128), F32),
        vmem((2, 2, 16, 128), F32), vmem((2, 2, 128), F32),
        vmem((2, N, 2, 16, 128), F32), vmem((2, N, 2, 128), F32),
        vmem((2, 2, 16, 128), F32), vmem((N, 2, 16, 128), F32),
        vmem((N, 64, 128), BF16), vmem((N, 8, 128), F32), vmem((N, 64, 128), BF16), vmem((N, 8, 128), F32),
        vmem((64, 128), BF16), vmem((8, 128), F32), vmem((N, 64, 128), BF16), vmem((N, 8, 128), F32),
        vmem((32, 128), BF16), vmem((N, 32, 128), BF16), vmem((256, 128), F32),
        pltpu.SemaphoreType.DMA((10,)), pltpu.SemaphoreType.DMA((17,)), pltpu.SemaphoreType.DMA((17,)),
        pltpu.SemaphoreType.DMA((N,)),
    ]
    return pl.pallas_call(
        kernel,
        name="step",
        out_shape=pltpu.VMEM((16, 32), BF16),
        in_specs=[pl.BlockSpec(memory_space=pl.ANY)] * len(operands),
        out_specs=pl.BlockSpec(memory_space=pltpu.VMEM),
        scratch_shapes=scratch,
        compiler_params=pltpu.CompilerParams(collective_id=0, has_side_effects=True),
    )(*operands)


def solution(mesh):
    in_specs = (
        P("dp", "kv"),
        P("kv"),
        P("kv", "tp"),
        P("tp"),
        P(),
        P("tp", "kv"),
        P("dp", "kv", None),
        P("dp", "kv", None),
        P("dp"),
    )
    return jax.shard_map(
        on_device, mesh=mesh, in_specs=in_specs, out_specs=P("dp", ("kv", "tp")), check_vma=False
    )
```

```python
import functools

import jax
import jax.numpy as jnp
import numpy as np
from jax import lax
from jax.experimental import pallas as pl
from jax.experimental.pallas import tpu as pltpu
from jax.sharding import PartitionSpec as P

D = 4096
EPS = 1e-05
NEG = -1e30
N = 8
FAR_FIRST = (4, 3, 5, 2, 6, 1, 7)
OWNERS = 7
MESH = pl.DeviceIdType.MESH
F32 = jnp.float32
BF16 = jnp.bfloat16


def kernel(
    tok_hbm, gain_hbm, wq_hbm, lam_hbm, hgain_hbm, wo_hbm, k_hbm, v_hbm, len_hbm, freq_hbm,
    out_ref,
    tok, gain, wq, lam, hgain, wo, kc, vc, lens, freq,
    qs, sqs, qr, sqr, zs, zsq, zr, zsqr, gs, gr,
    ns, ss, nr, sr, n2s, s2s, n2r, s2r, fs, fr, full,
    local_sem, send_sem, recv_sem, piece_sem,
):
    kv = lax.axis_index("kv")
    tp = lax.axis_index("tp")
    y = lax.rem(kv, N)
    z = lax.div(kv, N)
    last = N - 1

    def load(i, src, dst):
        return pltpu.make_async_copy(src, dst, local_sem.at[i])

    l_tok = load(0, tok_hbm, tok)
    l_gain = load(1, gain_hbm, gain)
    l_wq = load(2, wq_hbm, wq)
    l_wo = load(3, wo_hbm.at[pl.ds(pl.multiple_of(tp * 32, 32), 32), :], wo.at[tp])
    l_len = load(4, len_hbm, lens)
    l_freq = load(5, freq_hbm, freq)
    l_lam = load(6, lam_hbm, lam.at[tp])
    l_hgain = load(7, hgain_hbm, hgain)
    l_k = load(8, k_hbm, kc)
    l_v = load(9, v_hbm, vc)
    for copy in (l_tok, l_gain, l_wq):
        copy.start()

    def at(zp, yp, core):
        return {"kv": zp * N + yp, "tp": core}

    def y_id(d):
        return at(z, lax.rem(y + d, N), 1)

    def z_id(d):
        return at(lax.rem(z + d, N), y, 1)

    def z_id0(d):
        return at(lax.rem(z + d, N), y, 0)

    barrier = pltpu.get_barrier_semaphore()

    def greet(ident):
        pl.semaphore_signal(barrier, inc=1, device_id=ident, device_id_type=MESH)

    @pl.when((tp == 1) & (z < last))
    def _():
        for d in FAR_FIRST:
            greet(z_id(d))
            greet(y_id(d))
        for d in range(N):
            greet(z_id0(d))

    @pl.when((tp == 0) | (z == last))
    def _():
        greet({"tp": 1 - tp})

    @pl.when(tp == 1)
    def _():
        for copy in (l_len, l_freq, l_hgain, l_k, l_v):
            copy.start()

    l_lam.start()
    l_wo.start()

    def copy_to(phase, src, dst, ident):
        return pltpu.make_async_remote_copy(
            src_ref=src, dst_ref=dst, send_sem=send_sem.at[phase], recv_sem=recv_sem.at[phase],
            device_id=ident, device_id_type=MESH,
        )

    def arrived(phase, ref):
        copy_to(phase, ref, ref, z_id0(0)).wait_recv()

    def left(phase, ref):
        copy_to(phase, ref, ref, z_id0(0)).wait_send()

    l_tok.wait()
    l_gain.wait()
    x = tok[...].astype(F32)
    scaled_in = (x * gain[...]).astype(BF16)
    l_wq.wait()
    partial = jnp.dot(scaled_in, wq[...], preferred_element_type=F32)
    for h in range(8):
        qs[pl.ds(h, 16, stride=8), :] = partial[:, 128 * h : 128 * h + 128]
    squares = jnp.broadcast_to(jnp.sum(x * x, -1, keepdims=True), (2 * N, 128))
    for j in range(N):
        sqs[j] = squares[2 * j : 2 * j + 2]

    def rows_of(piece):
        if isinstance(piece, int):
            return pl.ds(piece * 16, 16)
        return pl.ds(pl.multiple_of(piece * 16, 16), 16)

    slot = tp * N + z

    def query_copy(d):
        piece = lax.rem(z + d, OWNERS)
        return copy_to(0, qs.at[rows_of(piece), :], qr.at[0, slot], at(piece, y, 1))

    def square_copy(d):
        piece = lax.rem(z + d, OWNERS)
        return copy_to(2, sqs.at[piece], sqr.at[0, z], at(piece, y, 1))

    def last_query_copy():
        return copy_to(1, qs.at[rows_of(last), :], qr.at[1, slot], at(0, y, 1))

    def last_square_copy():
        return copy_to(3, sqs.at[last], sqr.at[1, z], at(0, y, 1))

    other = {"tp": 1 - tp}
    swap_wo = copy_to(
        4, wo_hbm.at[pl.ds(pl.multiple_of((1 - tp) * 32, 32), 32), :], wo.at[tp], other
    )
    swap_lam = copy_to(5, lam_hbm, lam.at[tp], other)

    @pl.when(tp == 0)
    def _():
        pl.semaphore_wait(barrier, jnp.where(z == last, N, N - 1))

    @pl.when(tp == 1)
    def _():
        pl.semaphore_wait(barrier, jnp.where(z == last, N, 2 * N - 2))

    ORDER = (4, 3, 5, 2, 6, 1)
    for d in ORDER:
        query_copy(d).start()

    @pl.when((tp == 0) | (z == last))
    def _():
        query_copy(0).start()

    @pl.when((tp == 0) | (z > 0))
    def _():
        last_query_copy().start()

    @pl.when(tp == 1)
    def _():
        for d in ORDER:
            square_copy(d).start()

        @pl.when(z == last)
        def _():
            square_copy(0).start()

        @pl.when(z > 0)
        def _():
            last_square_copy().start()

    swap_lam.start()
    swap_wo.start()

    @pl.when(tp == 1)
    def _():
        lane = lax.broadcasted_iota(jnp.int32, (8, 128), 1)
        l_len.wait()
        l_freq.wait()

        def tables_of(piece):
            tables = []
            for b2 in range(2):
                position = (lens[2 * piece + b2] - 1).astype(F32)
                angles = position * jnp.broadcast_to(freq[...], (8, 128))
                tables.append((jnp.cos(angles), jnp.sin(angles)))
            return tables

        def plane_sum(i, piece):
            qr[i, N + z] = qs[rows_of(piece), :]
            sqr[i, z] = sqs[piece]
            arrived(i, qr.at[i, pl.ds(0, 2 * N - 1)])
            arrived(2 + i, sqr.at[i, pl.ds(0, N - 1)])
            for t in range(2):
                zs[i, t] = functools.reduce(lambda a, b: a + b, [qr[i, N * t + k] for k in range(N)])
            zsq[i] = functools.reduce(lambda a, b: a + b, [sqr[i, k] for k in range(N)])
            for d in FAR_FIRST:
                copy_to(6 + i, zs.at[i], zr.at[i, N - d], y_id(d)).start()
                copy_to(8 + i, zsq.at[i], zsqr.at[i, N - d], y_id(d)).start()

        def finished(i, piece, tables):
            arrived(6 + i, zr.at[i, pl.ds(1, N - 1)])
            arrived(8 + i, zsqr.at[i, pl.ds(1, N - 1)])
            total_sq = functools.reduce(lambda a, b: a + b, [zsqr[i, k] for k in range(1, N)], zsq[i])
            scale = lax.rsqrt(total_sq / D + EPS)
            for t in range(2):
                total = functools.reduce(lambda a, b: a + b, [zr[i, k, t] for k in range(1, N)], zs[i, t])
                for b2 in range(2):
                    cosine, sine = tables[b2]
                    q = total[8 * b2 : 8 * b2 + 8] * scale[b2 : b2 + 1]
                    turned = jnp.where((lane & 32) == 0, -pltpu.roll(q, 96, 1), pltpu.roll(q, 32, 1))
                    q = (q * cosine + turned * sine) * 0.125
                    gs[i, t, 8 * b2 : 8 * b2 + 8, :] = q
                    gr[piece, t, 8 * b2 : 8 * b2 + 8, :] = q
            for d in FAR_FIRST:
                pltpu.make_async_remote_copy(
                    src_ref=gs.at[i], dst_ref=gr.at[piece], send_sem=send_sem.at[10 + i],
                    recv_sem=piece_sem.at[piece], device_id=z_id(d), device_id_type=MESH,
                ).start()

        @pl.when((z > 0) & (z < last))
        def _():
            tables = tables_of(z)
            plane_sum(0, z)
            finished(0, z, tables)

        @pl.when(z == 0)
        def _():
            tables = tables_of(0)
            last_tables = tables_of(last)
            plane_sum(0, 0)
            plane_sum(1, last)
            finished(0, 0, tables)
            finished(1, last, last_tables)

        l_k.wait()
        l_v.wait()
        group = lane // 8
        diagonal = lax.rem(lane, 8) == lax.broadcasted_iota(jnp.int32, (8, 128), 0)
        positions = kv * 256 + lax.broadcasted_iota(jnp.int32, (32, 256), 1)

        def attend(d):
            piece = lax.rem(z + d, N)

            @pl.when(((piece != z) | (z == last)) & ((piece != last) | (z != 0)))
            def _():
                pltpu.make_async_remote_copy(
                    src_ref=gs.at[0], dst_ref=gr.at[piece], send_sem=send_sem.at[10],
                    recv_sem=piece_sem.at[piece], device_id=z_id0(0), device_id_type=MESH,
                ).wait_recv()

            stats = jnp.zeros((8, 128), F32)
            for b2 in range(2):
                b = 2 * piece + b2
                q = [gr[piece, t, 8 * b2 : 8 * b2 + 8, :] for t in range(2)]
                rows = jnp.concatenate(
                    [jnp.where(lane < 64, part, 0.0) for part in q]
                    + [jnp.where(lane < 64, 0.0, part) for part in q], 0
                )
                high = rows.astype(BF16)
                low = (rows - high.astype(F32)).astype(BF16)
                scores = lax.dot_general(
                    jnp.concatenate([high, low], 0), kc[b], (((1,), (1,)), ((), ())),
                    preferred_element_type=F32,
                )
                scores = scores[:32] + scores[32:]
                valid = positions < lens[b]
                scores = jnp.where(valid, scores, NEG)
                top = jnp.max(scores, -1, keepdims=True)
                weights = jnp.where(valid, jnp.exp(scores - top), 0.0)
                totals = jnp.sum(weights, -1, keepdims=True)
                numer = jnp.dot(weights.astype(BF16), vc[b], preferred_element_type=F32)
                ns[d, 32 * b2 : 32 * b2 + 32, :] = numer.astype(BF16)
                for i in range(4):
                    k = 4 * b2 + i
                    stats = jnp.where(group == k, top[8 * i : 8 * i + 8], stats)
                    stats = jnp.where(group == 8 + k, totals[8 * i : 8 * i + 8], stats)
            ss[d] = jnp.sum(jnp.where(diagonal, stats, 0.0), 0, keepdims=True)
            if d:
                copy_to(12, ss.at[d], sr.at[N - d], z_id(d)).start()
                copy_to(13, ns.at[d], nr.at[N - d], z_id(d)).start()

        for d in (7, 1, 6, 2, 5, 3, 4, 0):
            attend(d)

        def combined(phase, stats, numer, stat_slots, numer_slots):
            arrived(phase, stat_slots.at[pl.ds(1, N - 1)])
            stat = jnp.concatenate([stats] + [stat_slots[k] for k in range(1, N)], 0)
            top = jnp.max(stat, 0, keepdims=True)
            factors = jnp.exp(stat - top)
            total = jnp.sum(pltpu.roll(factors, 64, 1) * stat, 0, keepdims=True)
            columns = factors.T
            arrived(phase + 1, numer_slots.at[pl.ds(1, N - 1)])
            sums = [columns[8 * k : 8 * k + 8, :1] * numer[8 * k : 8 * k + 8] for k in range(8)]
            for i in range(1, N):
                block = numer_slots[i].astype(F32)
                for k in range(8):
                    sums[k] = sums[k] + columns[8 * k : 8 * k + 8, i : i + 1] * block[8 * k : 8 * k + 8]
            return jnp.where(lane[:1] < 64, top, total), sums

        stats, sums = combined(12, ss[0], ns[0].astype(F32), sr, nr)
        numer = jnp.concatenate(sums, 0)
        s2s[...] = stats
        n2s[...] = numer.astype(BF16)
        for d in FAR_FIRST:
            copy_to(14, s2s, s2r.at[N - d], y_id(d)).start()
            copy_to(15, n2s, n2r.at[N - d], y_id(d)).start()
        l_hgain.wait()
        l_lam.wait()
        arrived(5, lam.at[0])
        lambdas = [
            jnp.sum(jnp.where(diagonal[:, :8], jnp.broadcast_to(lam[t], (8, 8)), 0.0), -1, keepdims=True)
            for t in range(2)
        ]
        stats, sums = combined(14, stats, numer, s2r, n2r)
        totals = jnp.broadcast_to(stats, (8, 128)).T
        normed = []
        for b2 in range(2):
            for t in range(2):
                first, second = (
                    sums[k] / totals[64 + 8 * k : 72 + 8 * k, :1] for k in (4 * b2 + t, 4 * b2 + 2 + t)
                )
                head = first - lambdas[t] * second
                factor = lax.rsqrt(jnp.mean(head * head, -1, keepdims=True) + EPS)
                normed.append(head * factor * hgain[...])
        normed = jnp.concatenate(normed, 0).astype(BF16)
        fs[...] = normed
        for d in FAR_FIRST:
            copy_to(16, fs, fr.at[N - d], z_id0(d)).start()
            copy_to(16, fs, fr.at[N - d], z_id(d)).start()
        copy_to(16, fs, fr.at[0], z_id0(0)).start()
        fr[0] = normed

    @pl.when(tp == 1)
    def _():
        arrived(16, fr.at[pl.ds(1, N - 1)])

    @pl.when(tp == 0)
    def _():
        l_lam.wait()
        arrived(5, lam.at[0])
        arrived(16, fr)

    l_wo.wait()
    arrived(4, wo.at[0])
    for d in range(N):
        full[pl.ds(pl.multiple_of(lax.rem(z + d, N) * 32, 32), 32), :] = fr[d].astype(F32)
    mixed = jnp.zeros((16, 32), F32)
    for t in range(2):
        flat = jnp.concatenate([full[pl.ds(8 * t + h, 16, stride=16), :] for h in range(8)], 1)
        mixed = mixed + lax.dot_general(
            flat.astype(BF16), wo[t], (((1,), (1,)), ((), ())), preferred_element_type=F32
        )
    out_ref[...] = mixed.astype(BF16)

    left(4, wo.at[0])
    left(5, lam.at[0])
    @pl.when((tp == 0) | (z == last))
    def _():
        left(0, qr.at[0, pl.ds(0, OWNERS)])

    @pl.when((tp == 1) & (z < last))
    def _():
        left(0, qr.at[0, pl.ds(0, OWNERS - 1)])

    @pl.when((tp == 0) | (z > 0))
    def _():
        left(1, qr.at[1, 0])

    @pl.when(tp == 1)
    def _():
        @pl.when(z == last)
        def _():
            left(2, sqr.at[0, pl.ds(0, OWNERS)])

        @pl.when(z < last)
        def _():
            left(2, sqr.at[0, pl.ds(0, OWNERS - 1)])
            left(6, zr.at[0, pl.ds(1, N - 1)])
            left(8, zsqr.at[0, pl.ds(1, N - 1)])
            left(10, gr.at[pl.ds(1, N - 1)])

        @pl.when(z > 0)
        def _():
            left(3, sqr.at[1, 0])

        @pl.when(z == 0)
        def _():
            left(7, zr.at[1, pl.ds(1, N - 1)])
            left(9, zsqr.at[1, pl.ds(1, N - 1)])
            left(11, gr.at[pl.ds(1, N - 1)])

        left(12, sr.at[pl.ds(1, N - 1)])
        left(13, nr.at[pl.ds(1, N - 1)])
        left(14, s2r.at[pl.ds(1, N - 1)])
        left(15, n2r.at[pl.ds(1, N - 1)])
        left(16, fr.at[pl.ds(1, N - 1)])
        left(16, fr)


def on_device(tokens, norm_gain, w_query, lambda_head, head_gain, w_out, keys, values, lengths):
    frequency = 1.0 / 10000.0 ** (np.arange(32, dtype=np.float32) / np.float32(32))
    freq = jnp.asarray(np.tile(frequency.astype(np.float32), 4)[None, :])
    operands = (
        tokens, norm_gain[None, :], w_query, lambda_head[None, :], head_gain[None, :], w_out.T, keys, values,
        lengths, freq,
    )
    vmem = pltpu.VMEM
    local = [vmem(a.shape, a.dtype) for a in operands]
    local[3] = vmem((2, 1, 8), F32)
    local[5] = vmem((2, 32, 1024), BF16)
    local[8] = pltpu.SMEM((16,), jnp.int32)
    scratch = local + [
        vmem((128, 128), F32), vmem((N, 2, 128), F32),
        vmem((2, 2 * N, 16, 128), F32), vmem((2, N, 2, 128), F32),
        vmem((2, 2, 16, 128), F32), vmem((2, 2, 128), F32),
        vmem((2, N, 2, 16, 128), F32), vmem((2, N, 2, 128), F32),
        vmem((2, 2, 16, 128), F32), vmem((N, 2, 16, 128), F32),
        vmem((N, 64, 128), BF16), vmem((N, 1, 128), F32), vmem((N, 64, 128), BF16), vmem((N, 1, 128), F32),
        vmem((64, 128), BF16), vmem((1, 128), F32), vmem((N, 64, 128), BF16), vmem((N, 1, 128), F32),
        vmem((32, 128), BF16), vmem((N, 32, 128), BF16), vmem((256, 128), F32),
        pltpu.SemaphoreType.DMA((10,)), pltpu.SemaphoreType.DMA((17,)), pltpu.SemaphoreType.DMA((17,)),
        pltpu.SemaphoreType.DMA((N,)),
    ]
    return pl.pallas_call(
        kernel,
        name="step",
        out_shape=pltpu.VMEM((16, 32), BF16),
        in_specs=[pl.BlockSpec(memory_space=pl.ANY)] * len(operands),
        out_specs=pl.BlockSpec(memory_space=pltpu.VMEM),
        scratch_shapes=scratch,
        compiler_params=pltpu.CompilerParams(collective_id=0, has_side_effects=True),
    )(*operands)


def solution(mesh):
    in_specs = (
        P("dp", "kv"),
        P("kv"),
        P("kv", "tp"),
        P("tp"),
        P(),
        P("tp", "kv"),
        P("dp", "kv", None),
        P("dp", "kv", None),
        P("dp"),
    )
    return jax.shard_map(
        on_device, mesh=mesh, in_specs=in_specs, out_specs=P("dp", ("kv", "tp")), check_vma=False
    )
```

```python
import functools

import jax
import jax.numpy as jnp
import numpy as np
from jax import lax
from jax.experimental import pallas as pl
from jax.experimental.pallas import tpu as pltpu
from jax.sharding import PartitionSpec as P

D = 4096
EPS = 1e-05
NEG = -1e30
N = 8
FAR_FIRST = (4, 3, 5, 2, 6, 1, 7)
OWNERS = 7
MESH = pl.DeviceIdType.MESH
F32 = jnp.float32
BF16 = jnp.bfloat16


def kernel(
    tok_hbm, gain_hbm, wq_hbm, lam_hbm, hgain_hbm, wo_hbm, k_hbm, v_hbm, len_hbm, freq_hbm,
    out_ref,
    tok, gain, wq, lam, hgain, wo, kc, vc, lens, freq,
    qs, sqs, qr, sqr, zs, zsq, zr, zsqr, gs, gr,
    ns, ss, nr, sr, n2s, s2s, n2r, s2r, fs, fr, full,
    local_sem, send_sem, recv_sem, piece_sem,
):
    kv = lax.axis_index("kv")
    tp = lax.axis_index("tp")
    y = lax.rem(kv, N)
    z = lax.div(kv, N)
    last = N - 1

    def load(i, src, dst):
        return pltpu.make_async_copy(src, dst, local_sem.at[i])

    l_tok = load(0, tok_hbm, tok)
    l_gain = load(1, gain_hbm, gain)
    l_wq = load(2, wq_hbm, wq)
    l_wo = load(3, wo_hbm.at[pl.ds(pl.multiple_of(tp * 32, 32), 32), :], wo.at[tp])
    l_len = load(4, len_hbm, lens)
    l_freq = load(5, freq_hbm, freq)
    l_lam = load(6, lam_hbm, lam.at[tp])
    l_hgain = load(7, hgain_hbm, hgain)
    l_k = load(8, k_hbm, kc)
    l_v = load(9, v_hbm, vc)
    for copy in (l_tok, l_gain, l_wq):
        copy.start()

    def at(zp, yp, core):
        return {"kv": zp * N + yp, "tp": core}

    def y_id(d):
        return at(z, lax.rem(y + d, N), 1)

    def z_id(d):
        return at(lax.rem(z + d, N), y, 1)

    def z_id0(d):
        return at(lax.rem(z + d, N), y, 0)

    barrier = pltpu.get_barrier_semaphore()

    def greet(ident):
        pl.semaphore_signal(barrier, inc=1, device_id=ident, device_id_type=MESH)

    @pl.when((tp == 1) & (z < last))
    def _():
        for d in FAR_FIRST:
            greet(z_id(d))
            greet(y_id(d))
        for d in range(N):
            greet(z_id0(d))

    @pl.when((tp == 0) | (z == last))
    def _():
        greet({"tp": 1 - tp})

    @pl.when(tp == 1)
    def _():
        for copy in (l_len, l_freq, l_hgain, l_k, l_v):
            copy.start()

    l_lam.start()
    l_wo.start()

    def copy_to(phase, src, dst, ident):
        return pltpu.make_async_remote_copy(
            src_ref=src, dst_ref=dst, send_sem=send_sem.at[phase], recv_sem=recv_sem.at[phase],
            device_id=ident, device_id_type=MESH,
        )

    def arrived(phase, ref):
        copy_to(phase, ref, ref, z_id0(0)).wait_recv()

    def left(phase, ref):
        copy_to(phase, ref, ref, z_id0(0)).wait_send()

    l_tok.wait()
    l_gain.wait()
    x = tok[...].astype(F32)
    scaled_in = (x * gain[...]).astype(BF16)
    l_wq.wait()
    partial = jnp.dot(scaled_in, wq[...], preferred_element_type=F32)
    for h in range(8):
        qs[pl.ds(h, 16, stride=8), :] = partial[:, 128 * h : 128 * h + 128]
    squares = jnp.broadcast_to(jnp.sum(x * x, -1, keepdims=True), (2 * N, 128))
    for j in range(N):
        sqs[j] = squares[2 * j : 2 * j + 2]

    def rows_of(piece):
        if isinstance(piece, int):
            return pl.ds(piece * 16, 16)
        return pl.ds(pl.multiple_of(piece * 16, 16), 16)

    slot = tp * N + z

    def query_copy(d):
        piece = lax.rem(z + d, OWNERS)
        return copy_to(0, qs.at[rows_of(piece), :], qr.at[0, slot], at(piece, y, 1))

    def square_copy(d):
        piece = lax.rem(z + d, OWNERS)
        return copy_to(2, sqs.at[piece], sqr.at[0, z], at(piece, y, 1))

    def last_query_copy():
        return copy_to(1, qs.at[rows_of(last), :], qr.at[1, slot], at(0, y, 1))

    def last_square_copy():
        return copy_to(3, sqs.at[last], sqr.at[1, z], at(0, y, 1))

    other = {"tp": 1 - tp}
    swap_wo = copy_to(
        4, wo_hbm.at[pl.ds(pl.multiple_of((1 - tp) * 32, 32), 32), :], wo.at[tp], other
    )
    swap_lam = copy_to(5, lam_hbm, lam.at[tp], other)

    @pl.when(tp == 0)
    def _():
        pl.semaphore_wait(barrier, jnp.where(z == last, N, N - 1))

    @pl.when(tp == 1)
    def _():
        pl.semaphore_wait(barrier, jnp.where(z == last, N, 2 * N - 2))

    ORDER = (4, 3, 5, 2, 6, 1)
    for d in ORDER:
        query_copy(d).start()

    @pl.when((tp == 0) | (z == last))
    def _():
        query_copy(0).start()

    @pl.when((tp == 0) | (z > 0))
    def _():
        last_query_copy().start()

    @pl.when(tp == 1)
    def _():
        for d in ORDER:
            square_copy(d).start()

        @pl.when(z == last)
        def _():
            square_copy(0).start()

        @pl.when(z > 0)
        def _():
            last_square_copy().start()

    swap_lam.start()
    swap_wo.start()

    @pl.when(tp == 1)
    def _():
        lane = lax.broadcasted_iota(jnp.int32, (8, 128), 1)
        l_len.wait()
        l_freq.wait()

        def tables_of(piece):
            tables = []
            for b2 in range(2):
                position = (lens[2 * piece + b2] - 1).astype(F32)
                angles = position * jnp.broadcast_to(freq[...], (8, 128))
                tables.append((jnp.cos(angles), jnp.sin(angles)))
            return tables

        def plane_sum(i, piece):
            qr[i, N + z] = qs[rows_of(piece), :]
            sqr[i, z] = sqs[piece]
            arrived(i, qr.at[i, pl.ds(0, 2 * N - 1)])
            arrived(2 + i, sqr.at[i, pl.ds(0, N - 1)])
            for t in range(2):
                zs[i, t] = functools.reduce(lambda a, b: a + b, [qr[i, N * t + k] for k in range(N)])
            zsq[i] = functools.reduce(lambda a, b: a + b, [sqr[i, k] for k in range(N)])
            for d in FAR_FIRST:
                copy_to(6 + i, zs.at[i], zr.at[i, N - d], y_id(d)).start()
                copy_to(8 + i, zsq.at[i], zsqr.at[i, N - d], y_id(d)).start()

        def finished(i, piece, tables):
            arrived(6 + i, zr.at[i, pl.ds(1, N - 1)])
            arrived(8 + i, zsqr.at[i, pl.ds(1, N - 1)])
            total_sq = functools.reduce(lambda a, b: a + b, [zsqr[i, k] for k in range(1, N)], zsq[i])
            scale = lax.rsqrt(total_sq / D + EPS)
            for t in range(2):
                total = functools.reduce(lambda a, b: a + b, [zr[i, k, t] for k in range(1, N)], zs[i, t])
                for b2 in range(2):
                    cosine, sine = tables[b2]
                    q = total[8 * b2 : 8 * b2 + 8] * scale[b2 : b2 + 1]
                    turned = jnp.where((lane & 32) == 0, -pltpu.roll(q, 96, 1), pltpu.roll(q, 32, 1))
                    q = (q * cosine + turned * sine) * 0.125
                    gs[i, t, 8 * b2 : 8 * b2 + 8, :] = q
                    gr[piece, t, 8 * b2 : 8 * b2 + 8, :] = q
            for d in FAR_FIRST:
                pltpu.make_async_remote_copy(
                    src_ref=gs.at[i], dst_ref=gr.at[piece], send_sem=send_sem.at[10 + i],
                    recv_sem=piece_sem.at[piece], device_id=z_id(d), device_id_type=MESH,
                ).start()

        @pl.when((z > 0) & (z < last))
        def _():
            tables = tables_of(z)
            plane_sum(0, z)
            finished(0, z, tables)

        @pl.when(z == 0)
        def _():
            tables = tables_of(0)
            last_tables = tables_of(last)
            plane_sum(0, 0)
            plane_sum(1, last)
            finished(0, 0, tables)
            finished(1, last, last_tables)

        l_k.wait()
        l_v.wait()
        group = lane // 8
        diagonal = lax.rem(lane, 8) == lax.broadcasted_iota(jnp.int32, (8, 128), 0)
        positions = kv * 256 + lax.broadcasted_iota(jnp.int32, (32, 256), 1)

        def attend(d):
            piece = lax.rem(z + d, N)

            @pl.when(((piece != z) | (z == last)) & ((piece != last) | (z != 0)))
            def _():
                pltpu.make_async_remote_copy(
                    src_ref=gs.at[0], dst_ref=gr.at[piece], send_sem=send_sem.at[10],
                    recv_sem=piece_sem.at[piece], device_id=z_id0(0), device_id_type=MESH,
                ).wait_recv()

            stats = jnp.zeros((8, 128), F32)
            for b2 in range(2):
                b = 2 * piece + b2
                q = [gr[piece, t, 8 * b2 : 8 * b2 + 8, :] for t in range(2)]
                rows = jnp.concatenate(
                    [jnp.where(lane < 64, part, 0.0) for part in q]
                    + [jnp.where(lane < 64, 0.0, part) for part in q], 0
                )
                high = rows.astype(BF16)
                low = (rows - high.astype(F32)).astype(BF16)
                scores = lax.dot_general(
                    jnp.concatenate([high, low], 0), kc[b], (((1,), (1,)), ((), ())),
                    preferred_element_type=F32,
                )
                scores = scores[:32] + scores[32:]
                valid = positions < lens[b]
                scores = jnp.where(valid, scores, NEG)
                top = jnp.max(scores, -1, keepdims=True)
                weights = jnp.where(valid, jnp.exp(scores - top), 0.0)
                totals = jnp.sum(weights, -1, keepdims=True)
                numer = jnp.dot(weights.astype(BF16), vc[b], preferred_element_type=F32)
                ns[d, 32 * b2 : 32 * b2 + 32, :] = numer.astype(BF16)
                for i in range(4):
                    k = 4 * b2 + i
                    stats = jnp.where(group == k, top[8 * i : 8 * i + 8], stats)
                    stats = jnp.where(group == 8 + k, totals[8 * i : 8 * i + 8], stats)
            ss[d] = jnp.sum(jnp.where(diagonal, stats, 0.0), 0, keepdims=True)
            if d:
                copy_to(12, ss.at[d], sr.at[N - d], z_id(d)).start()
                copy_to(13, ns.at[d], nr.at[N - d], z_id(d)).start()

        for d in (7, 1, 6, 2, 5, 4, 3, 0):
            attend(d)

        def combined(phase, stats, numer, stat_slots, numer_slots):
            arrived(phase, stat_slots.at[pl.ds(1, N - 1)])
            stat = jnp.concatenate([stats] + [stat_slots[k] for k in range(1, N)], 0)
            top = jnp.max(stat, 0, keepdims=True)
            factors = jnp.exp(stat - top)
            total = jnp.sum(pltpu.roll(factors, 64, 1) * stat, 0, keepdims=True)
            columns = factors.T
            arrived(phase + 1, numer_slots.at[pl.ds(1, N - 1)])
            sums = [columns[8 * k : 8 * k + 8, :1] * numer[8 * k : 8 * k + 8] for k in range(8)]
            for i in range(1, N):
                block = numer_slots[i].astype(F32)
                for k in range(8):
                    sums[k] = sums[k] + columns[8 * k : 8 * k + 8, i : i + 1] * block[8 * k : 8 * k + 8]
            return jnp.where(lane[:1] < 64, top, total), sums

        stats, sums = combined(12, ss[0], ns[0].astype(F32), sr, nr)
        numer = jnp.concatenate(sums, 0)
        s2s[...] = stats
        n2s[...] = numer.astype(BF16)
        for d in FAR_FIRST:
            copy_to(14, s2s, s2r.at[N - d], y_id(d)).start()
            copy_to(15, n2s, n2r.at[N - d], y_id(d)).start()
        l_hgain.wait()
        l_lam.wait()
        arrived(5, lam.at[0])
        lambdas = [
            jnp.sum(jnp.where(diagonal[:, :8], jnp.broadcast_to(lam[t], (8, 8)), 0.0), -1, keepdims=True)
            for t in range(2)
        ]
        stats, sums = combined(14, stats, numer, s2r, n2r)
        totals = jnp.broadcast_to(stats, (8, 128)).T
        normed = []
        for b2 in range(2):
            for t in range(2):
                first, second = (
                    sums[k] / totals[64 + 8 * k : 72 + 8 * k, :1] for k in (4 * b2 + t, 4 * b2 + 2 + t)
                )
                head = first - lambdas[t] * second
                factor = lax.rsqrt(jnp.mean(head * head, -1, keepdims=True) + EPS)
                normed.append(head * factor * hgain[...])
        normed = jnp.concatenate(normed, 0).astype(BF16)
        fs[...] = normed
        for d in FAR_FIRST:
            copy_to(16, fs, fr.at[N - d], z_id0(d)).start()
            copy_to(16, fs, fr.at[N - d], z_id(d)).start()
        copy_to(16, fs, fr.at[0], z_id0(0)).start()
        fr[0] = normed

    @pl.when(tp == 1)
    def _():
        arrived(16, fr.at[pl.ds(1, N - 1)])

    @pl.when(tp == 0)
    def _():
        l_lam.wait()
        arrived(5, lam.at[0])
        arrived(16, fr)

    l_wo.wait()
    arrived(4, wo.at[0])
    for d in range(N):
        full[pl.ds(pl.multiple_of(lax.rem(z + d, N) * 32, 32), 32), :] = fr[d].astype(F32)
    mixed = jnp.zeros((16, 32), F32)
    for t in range(2):
        flat = jnp.concatenate([full[pl.ds(8 * t + h, 16, stride=16), :] for h in range(8)], 1)
        mixed = mixed + lax.dot_general(
            flat.astype(BF16), wo[t], (((1,), (1,)), ((), ())), preferred_element_type=F32
        )
    out_ref[...] = mixed.astype(BF16)

    left(4, wo.at[0])
    left(5, lam.at[0])
    @pl.when((tp == 0) | (z == last))
    def _():
        left(0, qr.at[0, pl.ds(0, OWNERS)])

    @pl.when((tp == 1) & (z < last))
    def _():
        left(0, qr.at[0, pl.ds(0, OWNERS - 1)])

    @pl.when((tp == 0) | (z > 0))
    def _():
        left(1, qr.at[1, 0])

    @pl.when(tp == 1)
    def _():
        @pl.when(z == last)
        def _():
            left(2, sqr.at[0, pl.ds(0, OWNERS)])

        @pl.when(z < last)
        def _():
            left(2, sqr.at[0, pl.ds(0, OWNERS - 1)])
            left(6, zr.at[0, pl.ds(1, N - 1)])
            left(8, zsqr.at[0, pl.ds(1, N - 1)])
            left(10, gr.at[pl.ds(1, N - 1)])

        @pl.when(z > 0)
        def _():
            left(3, sqr.at[1, 0])

        @pl.when(z == 0)
        def _():
            left(7, zr.at[1, pl.ds(1, N - 1)])
            left(9, zsqr.at[1, pl.ds(1, N - 1)])
            left(11, gr.at[pl.ds(1, N - 1)])

        left(12, sr.at[pl.ds(1, N - 1)])
        left(13, nr.at[pl.ds(1, N - 1)])
        left(14, s2r.at[pl.ds(1, N - 1)])
        left(15, n2r.at[pl.ds(1, N - 1)])
        left(16, fr.at[pl.ds(1, N - 1)])
        left(16, fr)


def on_device(tokens, norm_gain, w_query, lambda_head, head_gain, w_out, keys, values, lengths):
    frequency = 1.0 / 10000.0 ** (np.arange(32, dtype=np.float32) / np.float32(32))
    freq = jnp.asarray(np.tile(frequency.astype(np.float32), 4)[None, :])
    operands = (
        tokens, norm_gain[None, :], w_query, lambda_head[None, :], head_gain[None, :], w_out.T, keys, values,
        lengths, freq,
    )
    vmem = pltpu.VMEM
    local = [vmem(a.shape, a.dtype) for a in operands]
    local[3] = vmem((2, 1, 8), F32)
    local[5] = vmem((2, 32, 1024), BF16)
    local[8] = pltpu.SMEM((16,), jnp.int32)
    scratch = local + [
        vmem((128, 128), F32), vmem((N, 2, 128), F32),
        vmem((2, 2 * N, 16, 128), F32), vmem((2, N, 2, 128), F32),
        vmem((2, 2, 16, 128), F32), vmem((2, 2, 128), F32),
        vmem((2, N, 2, 16, 128), F32), vmem((2, N, 2, 128), F32),
        vmem((2, 2, 16, 128), F32), vmem((N, 2, 16, 128), F32),
        vmem((N, 64, 128), BF16), vmem((N, 1, 128), F32), vmem((N, 64, 128), BF16), vmem((N, 1, 128), F32),
        vmem((64, 128), BF16), vmem((1, 128), F32), vmem((N, 64, 128), BF16), vmem((N, 1, 128), F32),
        vmem((32, 128), BF16), vmem((N, 32, 128), BF16), vmem((256, 128), F32),
        pltpu.SemaphoreType.DMA((10,)), pltpu.SemaphoreType.DMA((17,)), pltpu.SemaphoreType.DMA((17,)),
        pltpu.SemaphoreType.DMA((N,)),
    ]
    return pl.pallas_call(
        kernel,
        name="step",
        out_shape=pltpu.VMEM((16, 32), BF16),
        in_specs=[pl.BlockSpec(memory_space=pl.ANY)] * len(operands),
        out_specs=pl.BlockSpec(memory_space=pltpu.VMEM),
        scratch_shapes=scratch,
        compiler_params=pltpu.CompilerParams(collective_id=0, has_side_effects=True),
    )(*operands)


def solution(mesh):
    in_specs = (
        P("dp", "kv"),
        P("kv"),
        P("kv", "tp"),
        P("tp"),
        P(),
        P("tp", "kv"),
        P("dp", "kv", None),
        P("dp", "kv", None),
        P("dp"),
    )
    return jax.shard_map(
        on_device, mesh=mesh, in_specs=in_specs, out_specs=P("dp", ("kv", "tp")), check_vma=False
    )
```
